128 devices in a mesh: ep: 32 (over z, y, core), tp: 4 (over x).
Axes of the slice: x: 4, y: 4, z: 4, core: 2. Of those that a mesh axis runs over, the one named last changes fastest.
Arguments:
- value_in: bfloat16 [16384, 2048], P('ep', 'tp'), may hold values from -400 to 400
- gate_in: bfloat16 [16384, 2048], P('ep', 'tp'), may hold values from -8 to 8
- conv_taps: float32 [31, 2048], P(None, 'tp'), may hold values from -1 to 1
- conv_bias: float32 [2048], P('tp'), may hold values from -3 to 3
- ln_gain: float32 [2048], P('tp'), may hold values from 0.1 to 1.9
- ln_bias: float32 [2048], P('tp'), may hold values from -3 to 3
- out_proj: bfloat16 [2048, 4096], P('tp'), may hold values from -0.125 to 0.125
- tokens_b: bfloat16 [16384, 4096], P('ep'), may hold values from -6 to 6
- norm_gain: float32 [4096], replicated, may hold values from 0.1 to 1.9
- routes: int32 [16384, 2], P(('ep', 'tp')), may hold values from 0 to 31, all different within a row; in each aligned block of 128 rows (0 to 127, 128 to 255, ...) at most 12 rows name the same one
- route_weights: float32 [16384, 2], P(('ep', 'tp')), may hold values from 0.2 to 1.5
- expert_gate: bfloat16 [32, 4096, 1024], P('ep', None, 'tp'), may hold values from -0.09375 to 0.09375
- expert_up: bfloat16 [32, 4096, 1024], P('ep', None, 'tp'), may hold values from -0.09375 to 0.09375
- expert_down: bfloat16 [32, 1024, 4096], P('ep', 'tp'), may hold values from -0.1875 to 0.1875
- shared_gate: bfloat16 [4096, 1024], P(None, 'tp'), may hold values from -0.09375 to 0.09375
- shared_up: bfloat16 [4096, 1024], P(None, 'tp'), may hold values from -0.09375 to 0.09375
- shared_down: bfloat16 [1024, 4096], P('tp'), may hold values from -0.1875 to 0.1875
Outputs:
- mixer_out: bfloat16 [16384, 4096], P(('ep', 'tp'))
- experts_out: bfloat16 [16384, 4096], P(('ep', 'tp'))
The draws below stay inside these ranges and needn't reach their ends.
Inputs may be any that keep to these rules, and one draw needn't show every extreme that they name: `routes`: each row names 2 different experts. In each aligned block of 128 rows (the rows of one device) no expert is named by more than 12 rows, and in some blocks an expert is named by exactly 12 rows.
All inputs are finite; a program needn't handle non-finite values.
Results may differ from the reference program's by a relative error of at most 0.012.
Values may be sent and summed in bfloat16 or wider, within the bound.
A program may use at most 128 MiB of HBM per device.

```python
import math
from functools import partial
import jax
import jax.numpy as jnp
import numpy as np
from jax import lax

D = 4096
CHANNELS = 2048
EXPERT_WIDTH = 1024
TAPS = 31
TOP_K = 2
ROWS_DEV = 128
EXPERTS = 32
CAP = 12
SEQ_LEN = 16384
TOKENS_B = 16384
N_TP = 4


def draw_value_in(key, part):
    keys = jax.random.split(jax.random.fold_in(key, 11), 2)
    base = jnp.clip(jax.random.normal(keys[0], (SEQ_LEN, CHANNELS), jnp.float32), -5.0, 5.0)
    column = jnp.arange(CHANNELS, dtype=jnp.float32) / CHANNELS
    rough = jax.random.uniform(keys[1], (CHANNELS,), jnp.float32, 0.5, 1.5)
    scales = 0.3 * 10.0 ** column * rough
    values = base * scales[None, :]
    return values.astype(jnp.bfloat16)


def levels(key, dims, shards, least, largest):
    gain, own = 1.0, jax.random.fold_in(key, 6)
    for position, shards_of in shards:
        draws = jnp.exp(jax.random.uniform(jax.random.fold_in(own, position), (shards_of,), jnp.float32, least / len(shards), largest / len(shards)))
        gain = gain * jnp.repeat(draws, dims[position] // shards_of).reshape([-1 if axis == position else 1 for axis in range(len(dims))])
    return gain


def deal_out(rng, own, number, rows, amount, top, limit, lean):
    order = jax.random.permutation(rng, amount)
    heavy_load, ordinary = load_shares(amount, rows * top, limit, lean, True), load_shares(amount, rows * top, limit, lean, False)
    places = jnp.arange(amount)

    def named(sizes, offset_by):
        used = int((sizes > 0).sum())
        fixed = max(1, used // 4)
        shifted = fixed + (places - fixed + offset_by * (used - fixed)) % max(1, amount - fixed)
        return jnp.zeros((amount,), jnp.int32).at[order[jnp.where(places < fixed, places, shifted)]].set(jnp.asarray(sizes, jnp.int32))

    sizes = jnp.where(number % 4 == 0, named(heavy_load, number // 4), named(ordinary, number - number // 4 - 1))
    mixed = jax.random.permutation(jax.random.fold_in(own, 3), amount)
    giver, sink = mixed[0:amount // 2 * 2:2], mixed[1:amount // 2 * 2:2]
    slack = jnp.minimum(sizes[giver] - 1, limit - sizes[sink]) // 2
    slack = jnp.where((giver == order[0]) | (sink == order[0]) | (sizes[sink] == 0), 0, jnp.maximum(slack, 0))
    shifted = jax.random.randint(jax.random.fold_in(own, 4), (amount // 2,), 0, 1 << 20) % (slack + 1)
    sizes = sizes.at[giver].add(-shifted).at[sink].add(shifted)
    labels = jnp.searchsorted(jnp.cumsum(sizes), jnp.arange(rows * top), side="right").astype(jnp.int32)
    table = labels.reshape(top, rows).T
    table = table[jax.random.permutation(jax.random.fold_in(own, 1), rows)]
    offset_by = jax.random.randint(jax.random.fold_in(own, 2), (rows, 1), 0, top)
    return jnp.take_along_axis(table, (jnp.arange(top)[None, :] + offset_by) % top, axis=1)


def load_shares(number_of, total, most, lean, full):
    portions = [(1 << 20) // math.isqrt(rank ** lean) + 1 for rank in range(1, number_of + 1)]
    largest = most if full else min(most, max(-(-total // number_of), total * portions[0] // sum(portions)))
    least = 1 if total - largest >= number_of - 1 else 0
    holding, rest = [largest] + [least] * (number_of - 1), total - largest - least * (number_of - 1)
    while rest > 0:
        free = [i for i in range(1, number_of) if holding[i] < largest] or [i for i in range(1, number_of) if holding[i] < most]
        whole, left = sum([portions[i] for i in free]), rest
        for i in free:
            addition = min(most - holding[i], max(1, left * portions[i] // whole), rest)
            holding[i] = holding[i] + addition
            rest = rest - addition
    return np.array(holding)


def normal_values(key, dims, deviation, bound, pieces=(), kind=jnp.bfloat16):
    values = jax.random.normal(key, dims, jnp.float32) * deviation
    if len(pieces) > 0:
        values = levels(key, dims, pieces, -0.22, 0.18) * values
    return jnp.clip(values, min=-bound, max=bound).astype(kind)


def setup_inputs(seed: int = 0) -> dict:
    key_of = jax.random.split(jax.random.key(seed), 18)
    value_in = draw_value_in(jax.random.fold_in(key_of[17], 71), 0)
    gate_in = normal_values(key_of[1], (SEQ_LEN, CHANNELS), 1.5, 8.0, ((0, 32), (1, 4)))
    conv_taps = normal_values(key_of[2], (TAPS, CHANNELS), TAPS ** -0.5, 1.0, ((1, 4),), jnp.float32)
    conv_bias = normal_values(key_of[3], (CHANNELS,), 0.5, 3.0, ((0, 4),), jnp.float32)
    ln_gain = jnp.clip(1.0 + 0.18 * jax.random.normal(key_of[4], (CHANNELS,), jnp.float32), 0.1, 1.9)
    ln_bias = normal_values(key_of[5], (CHANNELS,), 0.5, 3.0, ((0, 4),), jnp.float32)
    out_proj = normal_values(key_of[6], (CHANNELS, D), CHANNELS ** -0.5, 0.125, ((0, 4),))
    tokens_b = normal_values(key_of[7], (TOKENS_B, D), 1.0, 6.0, ((0, 32),))
    norm_gain = jnp.clip(1.0 + 0.18 * jax.random.normal(key_of[8], (D,), jnp.float32), 0.1, 1.9)
    routes_keys = jax.random.split(jax.random.fold_in(key_of[9], 1), TOKENS_B // ROWS_DEV)
    routes_turns = jax.random.permutation(jax.random.fold_in(key_of[9], 3), TOKENS_B // ROWS_DEV)
    routes = jax.vmap(lambda own, number: deal_out(jax.random.fold_in(key_of[9], 2), own, number, ROWS_DEV, EXPERTS, TOP_K, CAP, 1))(routes_keys, routes_turns).reshape((TOKENS_B, TOP_K))
    route_weights = jnp.clip(0.2 + 1.3 * jax.random.uniform(key_of[10], (TOKENS_B, TOP_K), jnp.float32) ** levels(key_of[10], (TOKENS_B, TOP_K), ((0, 128),), -0.2, 0.2), 0.2, 1.5)
    expert_gate = normal_values(key_of[11], (EXPERTS, D, EXPERT_WIDTH), D ** -0.5, 0.09375, ((0, 32), (2, 4)))
    expert_up = normal_values(key_of[12], (EXPERTS, D, EXPERT_WIDTH), D ** -0.5, 0.09375, ((0, 32), (2, 4)))
    expert_down = normal_values(key_of[13], (EXPERTS, EXPERT_WIDTH, D), EXPERT_WIDTH ** -0.5, 0.1875, ((0, 32), (1, 4)))
    shared_gate = normal_values(key_of[14], (D, EXPERT_WIDTH), D ** -0.5, 0.09375, ((1, 4),))
    shared_up = normal_values(key_of[15], (D, EXPERT_WIDTH), D ** -0.5, 0.09375, ((1, 4),))
    shared_down = normal_values(key_of[16], (EXPERT_WIDTH, D), EXPERT_WIDTH ** -0.5, 0.1875, ((0, 4),))
    return dict(value_in=value_in, gate_in=gate_in, conv_taps=conv_taps, conv_bias=conv_bias, ln_gain=ln_gain, ln_bias=ln_bias, out_proj=out_proj, tokens_b=tokens_b, norm_gain=norm_gain, routes=routes, route_weights=route_weights, expert_gate=expert_gate, expert_up=expert_up, expert_down=expert_down, shared_gate=shared_gate, shared_up=shared_up, shared_down=shared_down)


EPSILON = 1e-06

def round_trip(values):
    return lax.optimization_barrier(values.astype(jnp.bfloat16)).astype(jnp.float32)

def blocked_product(hidden, weight):
    block_rows = hidden.shape[1] // N_TP
    summed = jnp.zeros((hidden.shape[0], weight.shape[1]), jnp.float32)
    for block in range(N_TP):
        partial_sum = jnp.dot(hidden[:, block * block_rows:(block + 1) * block_rows], weight[block * block_rows:(block + 1) * block_rows], preferred_element_type=jnp.float32)
        summed = summed + round_trip(partial_sum)
    return summed.astype(jnp.bfloat16)

def gated_ffn(rows_in, weight_gate, weight_up, weight_down):
    hidden = (jax.nn.silu(jnp.dot(rows_in, weight_gate, preferred_element_type=jnp.float32)) * jnp.dot(rows_in, weight_up, preferred_element_type=jnp.float32)).astype(jnp.bfloat16)
    return blocked_product(hidden, weight_down)

def slot_table(route_ids, expert_count):
    chosen = route_ids.reshape(-1)
    onehot = (chosen[:, None] == jnp.arange(expert_count, dtype=jnp.int32)[None, :]).astype(jnp.int32)
    earlier = jnp.cumsum(onehot, axis=0) - onehot
    return (chosen, lax.optimization_barrier(jnp.sum(earlier * onehot, axis=1)).astype(jnp.int32))

def reference(value_in, gate_in, conv_taps, conv_bias, ln_gain, ln_bias, out_proj, tokens_b, norm_gain, routes, route_weights, expert_gate, expert_up, expert_down, shared_gate, shared_up, shared_down):
    gated = round_trip(value_in.astype(jnp.float32) * jax.nn.sigmoid(gate_in.astype(jnp.float32)))
    padded = jnp.concatenate([jnp.zeros((TAPS - 1, CHANNELS), jnp.float32), gated], axis=0)
    filtered = jnp.zeros((SEQ_LEN, CHANNELS), jnp.float32) + conv_bias[None, :]
    for tap_index in range(TAPS):
        filtered = filtered + conv_taps[tap_index][None, :] * padded[tap_index:tap_index + SEQ_LEN]
    average = lax.optimization_barrier(jnp.sum(filtered, axis=1)) / CHANNELS
    variance = lax.optimization_barrier(jnp.sum(filtered * filtered, axis=1)) / CHANNELS - average * average
    normed_a = (filtered - average[:, None]) * lax.rsqrt(variance[:, None] + EPSILON) * ln_gain + ln_bias
    activated = jax.nn.silu(normed_a).astype(jnp.bfloat16)
    mixer_out = blocked_product(activated, out_proj)
    features = tokens_b.astype(jnp.float32)
    normed_b = (features * lax.rsqrt(lax.optimization_barrier(jnp.mean(features * features, axis=1, keepdims=True)) + EPSILON) * norm_gain).astype(jnp.bfloat16)
    block_count = TOKENS_B // ROWS_DEV
    chosen, places = jax.vmap(partial(slot_table, expert_count=EXPERTS))(routes.reshape(block_count, ROWS_DEV * TOP_K))
    row_ids = jnp.arange(block_count, dtype=jnp.int32)[:, None] * ROWS_DEV + jnp.arange(ROWS_DEV * TOP_K, dtype=jnp.int32)[None, :] // TOP_K
    block_grid = jnp.broadcast_to(jnp.arange(block_count, dtype=jnp.int32)[:, None], row_ids.shape)
    slot_rows = jnp.zeros((EXPERTS, block_count, CAP), jnp.int32).at[chosen, block_grid, places].set(row_ids)
    slot_weights = jnp.zeros((EXPERTS, block_count, CAP), jnp.float32).at[chosen, block_grid, places].set(route_weights.reshape(block_count, ROWS_DEV * TOP_K))

    def per_expert(accumulated, inputs):
        weight_gate, weight_up, weight_down, rows_expert, weights_expert = inputs
        picked_ids = rows_expert.reshape(-1)
        outputs = gated_ffn(normed_b[picked_ids], weight_gate, weight_up, weight_down)
        accumulated = accumulated.at[picked_ids].add(outputs.astype(jnp.float32) * weights_expert.reshape(-1)[:, None])
        return (accumulated, None)
    routed, _ = lax.scan(per_expert, jnp.zeros((TOKENS_B, D), jnp.float32), (expert_gate, expert_up, expert_down, slot_rows, slot_weights))
    shared_rows = gated_ffn(normed_b, shared_gate, shared_up, shared_down)
    experts_out = (shared_rows.astype(jnp.float32) + routed).astype(jnp.bfloat16)
    return (mixer_out, experts_out)
```

```python
import functools

import jax
import jax.numpy as jnp
from jax import lax
from jax.experimental import pallas as pl
from jax.experimental.pallas import tpu as pltpu
from jax.sharding import PartitionSpec as P

EPSILON = 1e-06
MESH = pl.DeviceIdType.MESH
CAP = 12
BF = jnp.bfloat16
F32 = jnp.float32


def expert_kernel(
    outbox,
    gate,
    up,
    down,
    ret,
    inbox,
    hid,
    wdn,
    outs,
    acc,
    sem_local,
    ds,
    dr,
    fs,
    fr,
    hs,
    hr,
    ws,
    wr,
    rs,
    rr,
):
    me = lax.axis_index("ep")
    t = lax.axis_index("tp")
    z, y, c = me // 8, (me // 2) % 4, me % 2
    p = t % 2
    rows = outbox.shape[1]
    half = outbox.shape[2]
    group = 8 * rows
    units = gate.shape[1]
    width = wdn.shape[1]
    depth = gate.shape[0]

    def offset(i):
        dy = (i // 2) % 4
        return (i // 8 + dy) % 4, dy, i % 2

    def ahead(i):
        dz, dy, dc = offset(i)
        return ((z + dz) % 4) * 8 + ((y + dy) % 4) * 2 + (c + dc) % 2

    def behind(i):
        dz, dy, dc = offset(i)
        return ((z + 4 - dz) % 4) * 8 + ((y + 4 - dy) % 4) * 2 + (c + dc) % 2

    def column(j):
        return (t + j) % 4

    def features(q, size):
        return pl.ds(pl.multiple_of(q * size, size), size)

    barrier = pltpu.get_barrier_semaphore()
    for i in range(1, 32):
        pl.semaphore_signal(barrier, inc=1, device_id={"ep": ahead(i)}, device_id_type=MESH)
    for j in range(1, 4):
        pl.semaphore_signal(barrier, inc=1, device_id={"tp": column(j)}, device_id_type=MESH)
    pl.semaphore_wait(barrier, 34)

    def weight_copy(j):
        return pltpu.make_async_remote_copy(
            src_ref=down.at[:, features(column(j), width)],
            dst_ref=wdn.at[features(t, units), :],
            send_sem=ws.at[j],
            recv_sem=wr.at[j],
            device_id={"tp": column(j)},
            device_id_type=MESH,
        )

    own_weight = pltpu.make_async_copy(
        down.at[:, features(t, width)], wdn.at[features(t, units), :], sem_local.at[0]
    )
    own_rows = pltpu.make_async_copy(
        outbox.at[me], inbox.at[pl.ds(0, rows), features(p, half)], sem_local.at[1]
    )

    def dispatch(i):
        return pltpu.make_async_remote_copy(
            src_ref=outbox.at[ahead(i)],
            dst_ref=inbox.at[pl.ds(i * rows, rows), features(p, half)],
            send_sem=ds.at[i],
            recv_sem=dr.at[i],
            device_id={"ep": ahead(i)},
            device_id_type=MESH,
        )

    def forward(i):
        place = inbox.at[pl.ds(i * rows, rows), features(p, half)]
        return pltpu.make_async_remote_copy(
            src_ref=place,
            dst_ref=place,
            send_sem=fs.at[i],
            recv_sem=fr.at[i],
            device_id={"tp": column(1 if i % 2 == 0 else 3)},
            device_id_type=MESH,
        )

    def hidden_copy(g, j):
        place = hid.at[pl.ds(g * group, group), features(t, units)]
        return pltpu.make_async_remote_copy(
            src_ref=place,
            dst_ref=place,
            send_sem=hs.at[g, j],
            recv_sem=hr.at[g, j],
            device_id={"tp": column(j)},
            device_id_type=MESH,
        )

    def give_back(i):
        return pltpu.make_async_remote_copy(
            src_ref=outs.at[pl.ds(i * rows, rows), :],
            dst_ref=ret.at[me],
            send_sem=rs.at[i],
            recv_sem=rr.at[i],
            device_id={"ep": behind(i)},
            device_id_type=MESH,
        )

    own_back = pltpu.make_async_copy(outs.at[pl.ds(0, rows), :], ret.at[me], sem_local.at[2])

    own_rows.start()
    for i in range(1, 32):
        dispatch(i).start()
    own_weight.start()
    for j in range(1, 4):
        weight_copy(j).start()

    def receive(g):
        for i in range(8 * g, 8 * g + 8):
            if i == 0:
                own_rows.wait()
            else:
                dispatch(i).wait_recv()
            forward(i).start()

    def hidden(g):
        for i in range(8 * g, 8 * g + 8):
            forward(i).wait_recv()
        span = pl.ds(g * group, group)
        acc[...] = jnp.zeros_like(acc)
        step = 1024

        def body(k, carry):
            ks = pl.ds(pl.multiple_of(k * step, step), step)
            x = inbox[span, ks]
            acc[:, 0:units] += jnp.dot(x, gate[ks, :], preferred_element_type=F32)
            acc[:, units : 2 * units] += jnp.dot(x, up[ks, :], preferred_element_type=F32)
            return carry

        lax.fori_loop(0, depth // step, body, 0)
        a = acc[:, 0:units]
        hid[span, features(t, units)] = (
            a * (1.0 / (1.0 + jnp.exp(-a))) * acc[:, units : 2 * units]
        ).astype(BF)
        for j in range(1, 4):
            hidden_copy(g, j).start()

    def project(g):
        for j in range(1, 4):
            hidden_copy(g, j).wait_recv()
        span = pl.ds(g * group, group)
        step = 256

        def body(k, carry):
            ks = pl.ds(pl.multiple_of(k * step, step), step)
            outs[span, ks] = jnp.dot(
                hid[span, :], wdn[:, ks], preferred_element_type=F32
            ).astype(BF)
            return carry

        lax.fori_loop(0, width // step, body, 0)
        for i in range(8 * g, 8 * g + 8):
            if i == 0:
                own_back.start()
            else:
                give_back(i).start()

    receive(0)
    receive(1)
    hidden(0)
    receive(2)
    hidden(1)
    own_weight.wait()
    for j in range(1, 4):
        weight_copy(j).wait()
    project(0)
    receive(3)
    hidden(2)
    project(1)
    hidden(3)
    project(2)
    project(3)

    for i in range(1, 32):
        dispatch(i).wait_send()
    for i in range(32):
        forward(i).wait_send()
    for g in range(4):
        for j in range(1, 4):
            hidden_copy(g, j).wait_send()
    own_back.wait()
    for i in range(1, 32):
        give_back(i).wait()


def routed_rows(outbox, gate, up, down):
    count, rows, half = outbox.shape
    depth, units = gate.shape
    width = down.shape[1] // 4
    total = count * rows
    dma = pltpu.SemaphoreType.DMA
    vmem = pl.BlockSpec(memory_space=pltpu.VMEM)
    hbm = pl.BlockSpec(memory_space=pl.ANY)
    return pl.pallas_call(
        expert_kernel,
        out_shape=jax.ShapeDtypeStruct((count, rows, width), BF),
        in_specs=[hbm, vmem, vmem, hbm],
        out_specs=hbm,
        scratch_shapes=[
            pltpu.VMEM((total, depth), BF),
            pltpu.VMEM((total, 4 * units), BF),
            pltpu.VMEM((4 * units, width), BF),
            pltpu.VMEM((total, width), BF),
            pltpu.VMEM((total // 4, 2 * units), F32),
            dma((3,)),
            dma((32,)),
            dma((32,)),
            dma((32,)),
            dma((32,)),
            dma((4, 4)),
            dma((4, 4)),
            dma((4,)),
            dma((4,)),
            dma((32,)),
            dma((32,)),
        ],
        compiler_params=pltpu.CompilerParams(
            collective_id=0, has_side_effects=True, vmem_limit_bytes=56 * 1024 * 1024
        ),
        cost_estimate=pl.CostEstimate(
            flops=150_000_000_000, bytes_accessed=32 * 1024 * 1024, transcendentals=0
        ),
    )(outbox, gate, up, down)


def shifted(x, axis, by):
    devices = lax.axis_size(axis)
    pairs = [(i, i + by) for i in range(devices) if 0 <= i + by < devices]
    return lax.ppermute(x, axis, pairs)


def tap_filter(value_in, gate_in, conv_taps, conv_bias):
    gated = (value_in.astype(F32) * jax.nn.sigmoid(gate_in.astype(F32))).astype(BF)
    rim = conv_taps.shape[0] - 1
    length = gated.shape[0]
    before = shifted(gated[length - rim :], "ep", 1)
    padded = jnp.concatenate([before, gated], axis=0).astype(F32)
    filtered = jnp.zeros(gated.shape, F32) + conv_bias[None, :]
    for tap in range(rim + 1):
        filtered = filtered + conv_taps[tap][None, :] * padded[tap : tap + length]
    return filtered


def per_device(
    value_in,
    gate_in,
    conv_taps,
    conv_bias,
    ln_gain,
    ln_bias,
    out_proj,
    tokens_b,
    norm_gain,
    routes,
    route_weights,
    expert_gate,
    expert_up,
    expert_down,
    shared_gate,
    shared_up,
    shared_down,
):
    tp_count = lax.axis_size("tp")
    ep_count = lax.axis_size("ep")
    t = lax.axis_index("tp")
    rows_own, top_count = routes.shape
    rows_all = rows_own * tp_count
    model_width = tokens_b.shape[1]

    tables = lax.all_gather(
        jnp.concatenate([routes.astype(F32), route_weights], axis=1), "tp", axis=0
    )
    chosen = tables[:, :, :top_count].astype(jnp.int32).reshape(tp_count, -1)
    weights = tables[:, :, top_count:].reshape(rows_all, top_count)
    onehot = (chosen[:, :, None] == jnp.arange(ep_count, dtype=jnp.int32)).astype(BF)
    pairs = chosen.shape[1]
    lower = (
        jnp.arange(pairs, dtype=jnp.int32)[:, None] > jnp.arange(pairs, dtype=jnp.int32)[None, :]
    ).astype(BF)
    earlier = jnp.einsum("ij,bje->bie", lower, onehot, preferred_element_type=F32)
    places = jnp.sum(earlier * onehot.astype(F32), axis=2).astype(jnp.int32)
    slots = (
        chosen * (tp_count * CAP)
        + jnp.arange(tp_count, dtype=jnp.int32)[:, None] * CAP
        + places
    ).reshape(rows_all, top_count)
    slot_count = ep_count * tp_count * CAP

    features = tokens_b.astype(F32)
    normed_b = (
        features
        * lax.rsqrt(jnp.mean(features * features, axis=1, keepdims=True) + EPSILON)
        * norm_gain
    ).astype(BF)
    half = model_width // 2
    part = lax.dynamic_slice_in_dim(normed_b, (t % 2) * half, half, 1)
    ids = jnp.arange(slot_count, dtype=jnp.int32)
    select = (
        (ids[:, None] == slots[None, :, 0]) | (ids[:, None] == slots[None, :, 1])
    ).astype(BF)
    outbox = jnp.dot(select, part, preferred_element_type=F32).astype(BF)
    outbox = outbox.reshape(ep_count, tp_count * CAP, half)

    filtered = tap_filter(value_in, gate_in, conv_taps, conv_bias)
    sums = jnp.stack([jnp.sum(filtered, axis=1), jnp.sum(filtered * filtered, axis=1)])
    sums = jnp.sum(lax.all_gather(sums, "tp", axis=0), axis=0)
    channel_count = filtered.shape[1] * tp_count
    average = sums[0] / channel_count
    variance = sums[1] / channel_count - average * average
    normed_a = (filtered - average[:, None]) * lax.rsqrt(
        variance[:, None] + EPSILON
    ) * ln_gain + ln_bias
    activated = jax.nn.silu(normed_a).astype(BF)
    mixer_part = jnp.dot(activated, out_proj, preferred_element_type=F32).astype(BF)
    shared_hidden = (
        jax.nn.silu(jnp.dot(normed_b, shared_gate, preferred_element_type=F32))
        * jnp.dot(normed_b, shared_up, preferred_element_type=F32)
    ).astype(BF)
    shared_part = jnp.dot(shared_hidden, shared_down, preferred_element_type=F32).astype(BF)
    mixer_rows = lax.psum_scatter(mixer_part, "tp", scatter_dimension=0, tiled=True)
    shared_rows = lax.psum_scatter(shared_part, "tp", scatter_dimension=0, tiled=True)

    returned = routed_rows(outbox, expert_gate[0], expert_up[0], expert_down[0])
    returned = returned.reshape(slot_count, -1)
    spread = jnp.where(ids[None, :] == slots[:, 0:1], weights[:, 0:1], 0.0) + jnp.where(
        ids[None, :] == slots[:, 1:2], weights[:, 1:2], 0.0
    )
    high = spread.astype(BF)
    low = (spread - high.astype(F32)).astype(BF)
    combined = jnp.dot(high, returned, preferred_element_type=F32) + jnp.dot(
        low, returned, preferred_element_type=F32
    )
    quarters = lax.all_to_all(
        combined.astype(BF).reshape(tp_count, rows_own, -1), "tp", 0, 0, tiled=True
    )
    routed = jnp.moveaxis(quarters, 0, 1).reshape(rows_own, model_width)
    experts_out = (shared_rows.astype(F32) + routed.astype(F32)).astype(BF)
    return (mixer_rows, experts_out)


def solution(mesh):
    return jax.shard_map(
        per_device,
        mesh=mesh,
        in_specs=(
            P("ep", "tp"),
            P("ep", "tp"),
            P(None, "tp"),
            P("tp"),
            P("tp"),
            P("tp"),
            P("tp", None),
            P("ep", None),
            P(),
            P(("ep", "tp"), None),
            P(("ep", "tp"), None),
            P("ep", None, "tp"),
            P("ep", None, "tp"),
            P("ep", "tp", None),
            P(None, "tp"),
            P(None, "tp"),
            P("tp", None),
        ),
        out_specs=(P(("ep", "tp"), None), P(("ep", "tp"), None)),
        check_vma=False,
    )
```

```python
import functools

import jax
import jax.numpy as jnp
from jax import lax
from jax.experimental import pallas as pl
from jax.experimental.pallas import tpu as pltpu
from jax.sharding import PartitionSpec as P

EPSILON = 1e-06
MESH = pl.DeviceIdType.MESH
CAP = 12
BF = jnp.bfloat16
F32 = jnp.float32


def expert_kernel(
    outbox,
    normed,
    value_in,
    gate_in,
    taps,
    conv_bias,
    ln_gain,
    ln_bias,
    proj_in,
    gate_hbm,
    up_hbm,
    down,
    sgate_hbm,
    sup_hbm,
    sdown_hbm,
    ret,
    mixer_out,
    shared_out,
    inbox,
    hid,
    wdn,
    outs,
    acc,
    gate,
    up,
    padded,
    filt,
    act,
    rim,
    rim_out,
    stats,
    proj,
    nb,
    sgate,
    sup,
    sdown,
    shid,
    part,
    first,
    second,
    sem_local,
    cs,
    cr,
    ss,
    sr,
    qs,
    qr,
    ds,
    dr,
    fs,
    fr,
    hs,
    hr,
    ws,
    wr,
    rs,
    rr,
):
    me = lax.axis_index("ep")
    t = lax.axis_index("tp")
    z, y, c = me // 8, (me // 2) % 4, me % 2
    p = t % 2
    rows = outbox.shape[1]
    half = outbox.shape[2]
    group = 8 * rows
    units = gate.shape[1]
    width = wdn.shape[1]
    depth = gate.shape[0]

    def offset(i):
        dy = (i // 2) % 4
        return (i // 8 + dy) % 4, dy, i % 2

    def ahead(i):
        dz, dy, dc = offset(i)
        return ((z + dz) % 4) * 8 + ((y + dy) % 4) * 2 + (c + dc) % 2

    def behind(i):
        dz, dy, dc = offset(i)
        return ((z + 4 - dz) % 4) * 8 + ((y + 4 - dy) % 4) * 2 + (c + dc) % 2

    def column(j):
        return (t + j) % 4

    def features(q, size):
        return pl.ds(pl.multiple_of(q * size, size), size)

    loads = [
        pltpu.make_async_copy(a, b, sem_local.at[3 + n])
        for n, (a, b) in enumerate(
            [
                (normed, nb),
                (sgate_hbm, sgate),
                (sup_hbm, sup),
                (sdown_hbm, sdown),
                (proj_in, proj),
                (gate_hbm, gate),
                (up_hbm, up),
            ]
        )
    ]
    barrier = pltpu.get_barrier_semaphore()
    for i in range(1, 32):
        pl.semaphore_signal(barrier, inc=1, device_id={"ep": ahead(i)}, device_id_type=MESH)
    for j in range(1, 4):
        pl.semaphore_signal(barrier, inc=1, device_id={"tp": column(j)}, device_id_type=MESH)
    pl.semaphore_wait(barrier, 34)

    def weight_copy(j):
        return pltpu.make_async_remote_copy(
            src_ref=down.at[:, features(column(j), width)],
            dst_ref=wdn.at[features(t, units), :],
            send_sem=ws.at[j],
            recv_sem=wr.at[j],
            device_id={"tp": column(j)},
            device_id_type=MESH,
        )

    own_weight = pltpu.make_async_copy(
        down.at[:, features(t, width)], wdn.at[features(t, units), :], sem_local.at[0]
    )
    own_rows = pltpu.make_async_copy(
        outbox.at[me], inbox.at[pl.ds(0, rows), features(p, half)], sem_local.at[1]
    )

    def dispatch(i):
        return pltpu.make_async_remote_copy(
            src_ref=outbox.at[ahead(i)],
            dst_ref=inbox.at[pl.ds(i * rows, rows), features(p, half)],
            send_sem=ds.at[i],
            recv_sem=dr.at[i],
            device_id={"ep": ahead(i)},
            device_id_type=MESH,
        )

    def forward(i):
        place = inbox.at[pl.ds(i * rows, rows), features(p, half)]
        return pltpu.make_async_remote_copy(
            src_ref=place,
            dst_ref=place,
            send_sem=fs.at[i],
            recv_sem=fr.at[i],
            device_id={"tp": column(1 if i % 2 == 0 else 3)},
            device_id_type=MESH,
        )

    def hidden_copy(g, j):
        place = hid.at[pl.ds(g * group, group), features(t, units)]
        return pltpu.make_async_remote_copy(
            src_ref=place,
            dst_ref=place,
            send_sem=hs.at[g, j],
            recv_sem=hr.at[g, j],
            device_id={"tp": column(j)},
            device_id_type=MESH,
        )

    def give_back(i):
        return pltpu.make_async_remote_copy(
            src_ref=outs.at[pl.ds(i * rows, rows), :],
            dst_ref=ret.at[me],
            send_sem=rs.at[i],
            recv_sem=rr.at[i],
            device_id={"ep": behind(i)},
            device_id_type=MESH,
        )

    own_back = pltpu.make_async_copy(outs.at[pl.ds(0, rows), :], ret.at[me], sem_local.at[2])

    own_rows.start()
    for i in range(1, 32):
        dispatch(i).start()
    own_weight.start()
    for j in range(1, 4):
        weight_copy(j).start()
    for load in loads:
        load.start()

    length, channels = value_in.shape
    edge = rim.shape[0]
    tap_count = taps.shape[0]
    block = length // 4
    wide = nb.shape[1]

    rim_copy = pltpu.make_async_remote_copy(
        src_ref=rim_out,
        dst_ref=rim,
        send_sem=cs.at[0],
        recv_sem=cr.at[0],
        device_id={"ep": (me + 1) % 32},
        device_id_type=MESH,
    )

    def stats_copy(j):
        return pltpu.make_async_remote_copy(
            src_ref=stats.at[t],
            dst_ref=stats.at[t],
            send_sem=ss.at[j],
            recv_sem=sr.at[j],
            device_id={"tp": column(j)},
            device_id_type=MESH,
        )

    def tiles(count, size, body):
        def step(k, carry):
            body(pl.ds(pl.multiple_of(k * size, size), size))
            return carry

        lax.fori_loop(0, count, step, 0)

    def gated_tile(span):
        g = gate_in[span, :].astype(F32)
        v = value_in[span, :].astype(F32) * (1.0 / (1.0 + jnp.exp(-g)))
        padded[pl.ds(pl.multiple_of(span.start + edge, edge), 64), :] = v.astype(BF).astype(F32)

    tiles(length // 64, 64, gated_tile)
    rim_out[...] = padded[length : length + edge, :].astype(BF)
    rim_copy.start()

    def shared_expert():
        for load in loads[:4]:
            load.wait()
        acc[...] = jnp.zeros_like(acc)

        def inner(ks):
            x = nb[:, ks]
            acc[:, 0:units] += jnp.dot(x, sgate[ks, :], preferred_element_type=F32)
            acc[:, units : 2 * units] += jnp.dot(x, sup[ks, :], preferred_element_type=F32)

        tiles(depth // 1024, 1024, inner)
        a = acc[:, 0:units]
        shid[...] = (a * (1.0 / (1.0 + jnp.exp(-a))) * acc[:, units : 2 * units]).astype(BF)

        def outer(ks):
            r = jnp.dot(shid[...], sdown[:, ks], preferred_element_type=F32).astype(BF)
            for b in range(4):
                part[b, block : 2 * block, ks] = r[b * block : (b + 1) * block, :]

        tiles(wide // 512, 512, outer)

    def convolve():
        rim_copy.wait_recv()
        padded[0:edge, :] = jnp.where(me == 0, 0.0, rim[...].astype(F32))

        def strip(k, carry):
            for q in range(channels // 128):
                cols = slice(128 * q, 128 * q + 128)
                window = padded[pl.ds(pl.multiple_of(k * 64, 64), 64 + edge), cols]
                total = jnp.zeros((64, 128), F32) + conv_bias[:, cols]
                for rest in range(8):
                    turned = window[rest : rest + 56 + edge, :] if rest else window
                    for tap in range(tap_count):
                        at = edge + 1 - tap_count + tap
                        if at % 8 == rest:
                            base = at - rest
                            total = total + taps[tap : tap + 1, cols] * turned[base : base + 64, :]
                filt[pl.ds(pl.multiple_of(k * 64, 64), 64), cols] = total
            return carry

        lax.fori_loop(0, length // 64, strip, 0)
        lane = lax.broadcasted_iota(jnp.int32, (128, 128), 1)
        for b in range(length // 128):
            rs_ = slice(128 * b, 128 * b + 128)
            f = filt[rs_, :]
            both = jnp.where(
                lane == 0,
                jnp.sum(f, axis=1, keepdims=True),
                jnp.where(lane == 1, jnp.sum(f * f, axis=1, keepdims=True), 0.0),
            )
            stats[t, :, rs_] = both.T[0:8, :]
        for j in range(1, 4):
            stats_copy(j).start()

    def activate():
        for j in range(1, 4):
            stats_copy(j).wait_recv()
        whole = 4.0 * channels
        for b in range(length // 128):
            rs_ = slice(128 * b, 128 * b + 128)
            total = (stats[0, :, rs_] + stats[1, :, rs_]) + (stats[2, :, rs_] + stats[3, :, rs_])
            turned = jnp.concatenate([total, jnp.zeros((120, 128), F32)], axis=0).T
            average = turned[:, 0:1] / whole
            variance = turned[:, 1:2] / whole - average * average
            v = (filt[rs_, :] - average) * lax.rsqrt(variance + EPSILON) * ln_gain[...] + ln_bias[
                ...
            ]
            act[rs_, :] = (v / (1.0 + jnp.exp(-v))).astype(BF)

    def mix():
        loads[4].wait()

        def outer(ks):
            r = jnp.dot(act[...], proj[:, ks], preferred_element_type=F32).astype(BF)
            for b in range(4):
                part[b, 0:block, ks] = r[b * block : (b + 1) * block, :]

        tiles(wide // 512, 512, outer)

    wing = wide // 2
    right, left, across = column(1), column(3), column(2)

    def reduce_copy(n):
        source = [
            part.at[across, :, pl.ds(0, wing)],
            part.at[across, :, pl.ds(wing, wing)],
            part.at[right],
            part.at[left],
        ][n]
        target = [first.at[0], first.at[1], second.at[0], second.at[1]][n]
        return pltpu.make_async_remote_copy(
            src_ref=source,
            dst_ref=target,
            send_sem=qs.at[n],
            recv_sem=qr.at[n],
            device_id={"tp": right if n % 2 == 0 else left},
            device_id_type=MESH,
        )

    def reduce_start():
        reduce_copy(0).start()
        reduce_copy(1).start()

    def reduce_pass():
        for n, owner in ((0, right), (1, left)):
            reduce_copy(n).wait_recv()
            for k in range(wing // 512):
                ks = slice(n * wing + 512 * k, n * wing + 512 * k + 512)
                part[owner, :, ks] = (
                    part[owner, :, ks].astype(F32)
                    + first[n, :, 512 * k : 512 * k + 512].astype(F32)
                ).astype(BF)
            reduce_copy(n + 2).start()

    def reduce_end():
        reduce_copy(2).wait_recv()
        reduce_copy(3).wait_recv()

        def body(ks):
            second[0, :, ks] = (
                part[t, :, ks].astype(F32)
                + second[0, :, ks].astype(F32)
                + second[1, :, ks].astype(F32)
            ).astype(BF)

        tiles(wide // 512, 512, body)
        for piece in result:
            piece.start()

    result = [
        pltpu.make_async_copy(second.at[0, pl.ds(0, block)], mixer_out, sem_local.at[10]),
        pltpu.make_async_copy(second.at[0, pl.ds(block, block)], shared_out, sem_local.at[11]),
    ]

    def receive(g):
        for i in range(8 * g, 8 * g + 8):
            if i == 0:
                own_rows.wait()
            else:
                dispatch(i).wait_recv()
            forward(i).start()

    def hidden(g):
        for i in range(8 * g, 8 * g + 8):
            forward(i).wait_recv()
        span = pl.ds(g * group, group)
        acc[...] = jnp.zeros_like(acc)

        def body(ks):
            x = inbox[span, ks]
            acc[0:group, 0:units] += jnp.dot(x, gate[ks, :], preferred_element_type=F32)
            acc[0:group, units : 2 * units] += jnp.dot(x, up[ks, :], preferred_element_type=F32)

        tiles(depth // 1024, 1024, body)
        a = acc[0:group, 0:units]
        hid[span, features(t, units)] = (
            a * (1.0 / (1.0 + jnp.exp(-a))) * acc[0:group, units : 2 * units]
        ).astype(BF)
        for j in range(1, 4):
            hidden_copy(g, j).start()

    def project(g):
        for j in range(1, 4):
            hidden_copy(g, j).wait_recv()
        span = pl.ds(g * group, group)
        step = 256

        def body(k, carry):
            ks = pl.ds(pl.multiple_of(k * step, step), step)
            outs[span, ks] = jnp.dot(
                hid[span, :], wdn[:, ks], preferred_element_type=F32
            ).astype(BF)
            return carry

        lax.fori_loop(0, width // step, body, 0)
        for i in range(8 * g, 8 * g + 8):
            if i == 0:
                own_back.start()
            else:
                give_back(i).start()

    shared_expert()
    convolve()
    receive(0)
    activate()
    mix()
    reduce_start()
    receive(1)
    loads[5].wait()
    loads[6].wait()
    hidden(0)
    receive(2)
    hidden(1)
    own_weight.wait()
    for j in range(1, 4):
        weight_copy(j).wait()
    project(0)
    receive(3)
    hidden(2)
    project(1)
    hidden(3)
    project(2)
    project(3)
    reduce_pass()
    reduce_end()

    rim_copy.wait_send()
    for j in range(1, 4):
        stats_copy(j).wait_send()
    for n in range(4):
        reduce_copy(n).wait_send()
    for piece in result:
        piece.wait()

    for i in range(1, 32):
        dispatch(i).wait_send()
    for i in range(32):
        forward(i).wait_send()
    for g in range(4):
        for j in range(1, 4):
            hidden_copy(g, j).wait_send()
    own_back.wait()
    for i in range(1, 32):
        give_back(i).wait()


def routed_rows(outbox, normed, mixer, weights):
    count, rows, half = outbox.shape
    depth, units = weights[0].shape
    width = weights[2].shape[1] // 4
    total = count * rows
    length, channels = mixer[0].shape
    wide = weights[2].shape[1]
    block = length // 4
    dma = pltpu.SemaphoreType.DMA
    vmem = pl.BlockSpec(memory_space=pltpu.VMEM)
    hbm = pl.BlockSpec(memory_space=pl.ANY)
    return pl.pallas_call(
        expert_kernel,
        out_shape=(
            jax.ShapeDtypeStruct((count, rows, width), BF),
            jax.ShapeDtypeStruct((block, wide), BF),
            jax.ShapeDtypeStruct((block, wide), BF),
        ),
        in_specs=[hbm, hbm] + [vmem] * 6 + [hbm] * 7,
        out_specs=(hbm, hbm, hbm),
        scratch_shapes=[
            pltpu.VMEM((total, depth), BF),
            pltpu.VMEM((total, 4 * units), BF),
            pltpu.VMEM((4 * units, width), BF),
            pltpu.VMEM((total, width), BF),
            pltpu.VMEM((length, 2 * units), F32),
            pltpu.VMEM((depth, units), BF),
            pltpu.VMEM((depth, units), BF),
            pltpu.VMEM((length + 32, channels), F32),
            pltpu.VMEM((length, channels), F32),
            pltpu.VMEM((length, channels), BF),
            pltpu.VMEM((32, channels), BF),
            pltpu.VMEM((32, channels), BF),
            pltpu.VMEM((4, 8, length), F32),
            pltpu.VMEM((channels, wide), BF),
            pltpu.VMEM((length, wide), BF),
            pltpu.VMEM((depth, units), BF),
            pltpu.VMEM((depth, units), BF),
            pltpu.VMEM((units, wide), BF),
            pltpu.VMEM((length, units), BF),
            pltpu.VMEM((4, 2 * block, wide), BF),
            pltpu.VMEM((2, 2 * block, wide // 2), BF),
            pltpu.VMEM((2, 2 * block, wide), BF),
            dma((12,)),
            dma((1,)),
            dma((1,)),
            dma((4,)),
            dma((4,)),
            dma((4,)),
            dma((4,)),
            dma((32,)),
            dma((32,)),
            dma((32,)),
            dma((32,)),
            dma((4, 4)),
            dma((4, 4)),
            dma((4,)),
            dma((4,)),
            dma((32,)),
            dma((32,)),
        ],
        compiler_params=pltpu.CompilerParams(
            collective_id=0, has_side_effects=True, vmem_limit_bytes=67_043_328
        ),
    )(outbox, normed, *mixer, *weights)


def per_device(
    value_in,
    gate_in,
    conv_taps,
    conv_bias,
    ln_gain,
    ln_bias,
    out_proj,
    tokens_b,
    norm_gain,
    routes,
    route_weights,
    expert_gate,
    expert_up,
    expert_down,
    shared_gate,
    shared_up,
    shared_down,
):
    tp_count = lax.axis_size("tp")
    ep_count = lax.axis_size("ep")
    t = lax.axis_index("tp")
    rows_own, top_count = routes.shape
    rows_all = rows_own * tp_count
    model_width = tokens_b.shape[1]

    tables = lax.all_gather(
        jnp.concatenate([routes.astype(F32), route_weights], axis=1), "tp", axis=0
    )
    chosen = tables[:, :, :top_count].astype(jnp.int32).reshape(tp_count, -1)
    weights = tables[:, :, top_count:].reshape(rows_all, top_count)
    onehot = (chosen[:, :, None] == jnp.arange(ep_count, dtype=jnp.int32)).astype(BF)
    pairs = chosen.shape[1]
    lower = (
        jnp.arange(pairs, dtype=jnp.int32)[:, None] > jnp.arange(pairs, dtype=jnp.int32)[None, :]
    ).astype(BF)
    earlier = jnp.einsum("ij,bje->bie", lower, onehot, preferred_element_type=F32)
    places = jnp.sum(earlier * onehot.astype(F32), axis=2).astype(jnp.int32)
    slots = (
        chosen * (tp_count * CAP)
        + jnp.arange(tp_count, dtype=jnp.int32)[:, None] * CAP
        + places
    ).reshape(rows_all, top_count)
    slot_count = ep_count * tp_count * CAP

    features = tokens_b.astype(F32)
    normed_b = (
        features
        * lax.rsqrt(jnp.mean(features * features, axis=1, keepdims=True) + EPSILON)
        * norm_gain
    ).astype(BF)
    half = model_width // 2
    part = lax.dynamic_slice_in_dim(normed_b, (t % 2) * half, half, 1)
    ids = jnp.arange(slot_count, dtype=jnp.int32)
    select = (
        (ids[:, None] == slots[None, :, 0]) | (ids[:, None] == slots[None, :, 1])
    ).astype(BF)
    outbox = jnp.dot(select, part, preferred_element_type=F32).astype(BF)
    outbox = outbox.reshape(ep_count, tp_count * CAP, half)

    returned, mixer_rows, shared_rows = routed_rows(
        outbox,
        normed_b,
        (
            value_in,
            gate_in,
            conv_taps,
            conv_bias[None, :],
            ln_gain[None, :],
            ln_bias[None, :],
            out_proj,
        ),
        (
            expert_gate[0],
            expert_up[0],
            expert_down[0],
            shared_gate,
            shared_up,
            shared_down,
        ),
    )
    returned = returned.reshape(slot_count, -1)
    spread = jnp.where(ids[None, :] == slots[:, 0:1], weights[:, 0:1], 0.0) + jnp.where(
        ids[None, :] == slots[:, 1:2], weights[:, 1:2], 0.0
    )
    high = spread.astype(BF)
    low = (spread - high.astype(F32)).astype(BF)
    combined = jnp.dot(high, returned, preferred_element_type=F32) + jnp.dot(
        low, returned, preferred_element_type=F32
    )
    quarters = lax.all_to_all(
        combined.astype(BF).reshape(tp_count, rows_own, -1), "tp", 0, 0, tiled=True
    )
    routed = jnp.moveaxis(quarters, 0, 1).reshape(rows_own, model_width)
    experts_out = (shared_rows.astype(F32) + routed.astype(F32)).astype(BF)
    return (mixer_rows, experts_out)


def solution(mesh):
    return jax.shard_map(
        per_device,
        mesh=mesh,
        in_specs=(
            P("ep", "tp"),
            P("ep", "tp"),
            P(None, "tp"),
            P("tp"),
            P("tp"),
            P("tp"),
            P("tp", None),
            P("ep", None),
            P(),
            P(("ep", "tp"), None),
            P(("ep", "tp"), None),
            P("ep", None, "tp"),
            P("ep", None, "tp"),
            P("ep", "tp", None),
            P(None, "tp"),
            P(None, "tp"),
            P("tp", None),
        ),
        out_specs=(P(("ep", "tp"), None), P(("ep", "tp"), None)),
        check_vma=False,
    )
```

```python
import functools

import jax
import jax.numpy as jnp
from jax import lax
from jax.experimental import pallas as pl
from jax.experimental.pallas import tpu as pltpu
from jax.sharding import PartitionSpec as P

EPSILON = 1e-06
MESH = pl.DeviceIdType.MESH
CAP = 12
EDGE = 1024
PAIRS = [
    (0, 0), (0, 1), (1, 0), (0, 3),
    (3, 0), (1, 1), (3, 1), (0, 2),
    (2, 0), (2, 1), (1, 3), (3, 3),
    (2, 3), (1, 2), (3, 2), (2, 2),
]
TURNS = [n for n, (a, b) in enumerate(PAIRS) if a and b]
STRAIGHT = [n for n, (a, b) in enumerate(PAIRS) if (a or b) and not (a and b)]
BF = jnp.bfloat16
F32 = jnp.float32


def expert_kernel(
    outbox,
    normed,
    value_in,
    gate_in,
    taps,
    conv_bias,
    ln_gain,
    ln_bias,
    proj_in,
    gate_hbm,
    up_hbm,
    down,
    sgate_hbm,
    sup_hbm,
    sdown_hbm,
    ret,
    mixer_out,
    shared_out,
    corner,
    corner_back,
    inbox,
    hid,
    wdn,
    outs,
    acc,
    gate,
    up,
    padded,
    filt,
    act,
    rim,
    rim_out,
    stats,
    proj,
    nb,
    sgate,
    sup,
    sdown,
    shid,
    part,
    first,
    second,
    sem_local,
    cs,
    cr,
    ss,
    sr,
    qs,
    qr,
    ds,
    dr,
    fs,
    fr,
    hs,
    hr,
    ws,
    wr,
    rs,
    rr,
    ks,
    kr,
    bs,
    br,
):
    me = lax.axis_index("ep")
    t = lax.axis_index("tp")
    z, y, c = me // 8, (me // 2) % 4, me % 2
    p = t % 2
    rows = outbox.shape[1]
    sent = outbox.shape[2]
    rest = gate.shape[0] - sent
    mine = pl.ds(pl.multiple_of((1 - p) * rest, 128), sent)
    lacking = pl.ds(pl.multiple_of((1 - p) * sent, 128), rest)
    group = 8 * rows
    units = gate.shape[1]
    width = wdn.shape[1]
    depth = gate.shape[0]

    def away(dz, dy, dc):
        return ((z + 4 + dz) % 4) * 8 + ((y + 4 + dy) % 4) * 2 + (c + dc) % 2

    def ahead(i):
        dz, dy = PAIRS[i // 2]
        return away(dz, dy, i % 2)

    def behind(i):
        dz, dy = PAIRS[i // 2]
        return away(-dz, -dy, i % 2)

    def legs(n):
        dz, dy = PAIRS[n]
        return ((0, dy), (dz, 0)) if (dz + dy) % 2 == 0 else ((dz, 0), (0, dy))

    def column(j):
        return (t + j) % 4

    def features(q, size):
        return pl.ds(pl.multiple_of(q * size, size), size)

    loads = [
        pltpu.make_async_copy(a, b, sem_local.at[3 + n])
        for n, (a, b) in enumerate(
            [
                (normed, nb),
                (sgate_hbm, sgate),
                (sup_hbm, sup),
                (sdown_hbm, sdown),
                (proj_in, proj),
                (gate_hbm, gate),
                (up_hbm, up),
            ]
        )
    ]
    barrier = pltpu.get_barrier_semaphore()
    for i in range(1, 32):
        pl.semaphore_signal(barrier, inc=1, device_id={"ep": ahead(i)}, device_id_type=MESH)
    for j in range(1, 4):
        pl.semaphore_signal(barrier, inc=1, device_id={"tp": column(j)}, device_id_type=MESH)
    pl.semaphore_wait(barrier, 34)

    def weight_copy(j):
        return pltpu.make_async_remote_copy(
            src_ref=down.at[:, features(column(j), width)],
            dst_ref=wdn.at[features(t, units), :],
            send_sem=ws.at[j],
            recv_sem=wr.at[j],
            device_id={"tp": column(j)},
            device_id_type=MESH,
        )

    own_weight = pltpu.make_async_copy(
        down.at[:, features(t, width)], wdn.at[features(t, units), :], sem_local.at[0]
    )
    own_rows = pltpu.make_async_copy(
        outbox.at[me], inbox.at[pl.ds(0, rows), mine], sem_local.at[1]
    )

    def dispatch(i):
        return pltpu.make_async_remote_copy(
            src_ref=outbox.at[ahead(i)],
            dst_ref=inbox.at[pl.ds(i * rows, rows), mine],
            send_sem=ds.at[i],
            recv_sem=dr.at[i],
            device_id={"ep": ahead(i)},
            device_id_type=MESH,
        )

    def to_corner(n):
        dz, dy = PAIRS[n]
        start = ((z + dz) % 4) * 8 + ((y + dy) % 4) * 2
        k = TURNS.index(n)
        leg = legs(n)[0]
        return pltpu.make_async_remote_copy(
            src_ref=outbox.at[pl.ds(start, 2)],
            dst_ref=corner.at[k],
            send_sem=ks.at[k],
            recv_sem=kr.at[k],
            device_id={"ep": away(*leg, 0)},
            device_id_type=MESH,
        )

    def from_corner(i):
        k = TURNS.index(i // 2)
        leg = legs(i // 2)[1]
        return pltpu.make_async_remote_copy(
            src_ref=corner.at[k, (c + i % 2) % 2],
            dst_ref=inbox.at[pl.ds(i * rows, rows), mine],
            send_sem=ds.at[i],
            recv_sem=dr.at[i],
            device_id={"ep": away(*leg, i % 2)},
            device_id_type=MESH,
        )

    def arrival(i):
        return from_corner(i) if i // 2 in TURNS else dispatch(i)

    def back_to_corner(n):
        k = TURNS.index(n)
        leg = legs(n)[0]
        return pltpu.make_async_remote_copy(
            src_ref=outs.at[pl.ds(n * 2 * rows, 2 * rows), :],
            dst_ref=corner_back.at[k],
            send_sem=bs.at[k],
            recv_sem=br.at[k],
            device_id={"ep": away(-leg[0], -leg[1], 0)},
            device_id_type=MESH,
        )

    def back_from_corner(i):
        k = TURNS.index(i // 2)
        one, two = legs(i // 2)
        return pltpu.make_async_remote_copy(
            src_ref=corner_back.at[k, pl.ds((i % 2) * rows, rows)],
            dst_ref=ret.at[away(*one, 0)],
            send_sem=rs.at[i],
            recv_sem=rr.at[i],
            device_id={"ep": away(-two[0], -two[1], i % 2)},
            device_id_type=MESH,
        )

    def return_leg(i):
        return back_from_corner(i) if i // 2 in TURNS else give_back(i)

    def forward(i):
        place = inbox.at[pl.ds(i * rows, rows), lacking]
        return pltpu.make_async_remote_copy(
            src_ref=place,
            dst_ref=place,
            send_sem=fs.at[i],
            recv_sem=fr.at[i],
            device_id={"tp": column(1 if i % 2 == 0 else 3)},
            device_id_type=MESH,
        )

    def hidden_copy(g, j):
        to = j
        source = t
        if j == 2:
            to = 1 if g % 2 == 0 else 3
            source = column(4 - to)
        place = hid.at[pl.ds(g * group, group), features(source, units)]
        return pltpu.make_async_remote_copy(
            src_ref=place,
            dst_ref=place,
            send_sem=hs.at[g, j],
            recv_sem=hr.at[g, j],
            device_id={"tp": column(to)},
            device_id_type=MESH,
        )

    def give_back(i):
        return pltpu.make_async_remote_copy(
            src_ref=outs.at[pl.ds(i * rows, rows), :],
            dst_ref=ret.at[me],
            send_sem=rs.at[i],
            recv_sem=rr.at[i],
            device_id={"ep": behind(i)},
            device_id_type=MESH,
        )

    own_back = pltpu.make_async_copy(outs.at[pl.ds(0, rows), :], ret.at[me], sem_local.at[2])

    own_rows.start()
    dispatch(1).start()
    straight = list(STRAIGHT)
    for count, n in enumerate(TURNS):
        to_corner(n).start()
        if count % 3 == 0:
            for _ in range(2):
                m = straight.pop(0)
                dispatch(2 * m).start()
                dispatch(2 * m + 1).start()
    own_weight.start()
    for j in range(1, 4):
        weight_copy(j).start()
    for load in loads:
        load.start()

    length, channels = value_in.shape
    edge = rim.shape[0]
    tap_count = taps.shape[0]
    block = length // 4
    wide = nb.shape[1]

    rim_copy = pltpu.make_async_remote_copy(
        src_ref=rim_out,
        dst_ref=rim,
        send_sem=cs.at[0],
        recv_sem=cr.at[0],
        device_id={"ep": (me + 1) % 32},
        device_id_type=MESH,
    )

    def stats_copy(j):
        return pltpu.make_async_remote_copy(
            src_ref=stats.at[t],
            dst_ref=stats.at[t],
            send_sem=ss.at[j],
            recv_sem=sr.at[j],
            device_id={"tp": column(j)},
            device_id_type=MESH,
        )

    def tiles(count, size, body):
        def step(k, carry):
            body(pl.ds(pl.multiple_of(k * size, size), size))
            return carry

        lax.fori_loop(0, count, step, 0)

    def gated_tile(span):
        g = gate_in[span, :].astype(F32)
        v = value_in[span, :].astype(F32) * (1.0 / (1.0 + jnp.exp(-g)))
        padded[pl.ds(pl.multiple_of(span.start + edge, edge), 64), :] = v.astype(BF).astype(F32)

    tiles(length // 64, 64, gated_tile)
    rim_out[...] = padded[length : length + edge, :].astype(BF)
    rim_copy.start()

    def shared_expert():
        for load in loads[:4]:
            load.wait()
        acc[...] = jnp.zeros_like(acc)

        def inner(ks):
            x = nb[:, ks]
            acc[:, 0:units] += jnp.dot(x, sgate[ks, :], preferred_element_type=F32)
            acc[:, units : 2 * units] += jnp.dot(x, sup[ks, :], preferred_element_type=F32)

        tiles(depth // 1024, 1024, inner)
        a = acc[:, 0:units]
        shid[...] = (a * (1.0 / (1.0 + jnp.exp(-a))) * acc[:, units : 2 * units]).astype(BF)

        def outer(ks):
            r = jnp.dot(shid[...], sdown[:, ks], preferred_element_type=F32).astype(BF)
            for b in range(4):
                part[b, block : 2 * block, ks] = r[b * block : (b + 1) * block, :]

        tiles(wide // 512, 512, outer)

    def convolve():
        rim_copy.wait_recv()
        padded[0:edge, :] = jnp.where(me == 0, 0.0, rim[...].astype(F32))

        def strip(k, carry):
            for q in range(channels // 128):
                cols = slice(128 * q, 128 * q + 128)
                window = padded[pl.ds(pl.multiple_of(k * 64, 64), 64 + edge), cols]
                total = jnp.zeros((64, 128), F32) + conv_bias[:, cols]
                for rest in range(8):
                    turned = window[rest : rest + 56 + edge, :] if rest else window
                    for tap in range(tap_count):
                        at = edge + 1 - tap_count + tap
                        if at % 8 == rest:
                            base = at - rest
                            total = total + taps[tap : tap + 1, cols] * turned[base : base + 64, :]
                filt[pl.ds(pl.multiple_of(k * 64, 64), 64), cols] = total
            return carry

        lax.fori_loop(0, length // 64, strip, 0)
        lane = lax.broadcasted_iota(jnp.int32, (128, 128), 1)
        for b in range(length // 128):
            rs_ = slice(128 * b, 128 * b + 128)
            f = filt[rs_, :]
            both = jnp.where(
                lane == 0,
                jnp.sum(f, axis=1, keepdims=True),
                jnp.where(lane == 1, jnp.sum(f * f, axis=1, keepdims=True), 0.0),
            )
            stats[t, :, rs_] = both.T[0:8, :]
        for j in range(1, 4):
            stats_copy(j).start()

    def activate():
        for j in range(1, 4):
            stats_copy(j).wait_recv()
        whole = 4.0 * channels
        for b in range(length // 128):
            rs_ = slice(128 * b, 128 * b + 128)
            total = (stats[0, :, rs_] + stats[1, :, rs_]) + (stats[2, :, rs_] + stats[3, :, rs_])
            turned = jnp.concatenate([total, jnp.zeros((120, 128), F32)], axis=0).T
            average = turned[:, 0:1] / whole
            variance = turned[:, 1:2] / whole - average * average
            v = (filt[rs_, :] - average) * lax.rsqrt(variance + EPSILON) * ln_gain[...] + ln_bias[
                ...
            ]
            act[rs_, :] = (v / (1.0 + jnp.exp(-v))).astype(BF)

    def mix():
        loads[4].wait()

        def outer(ks):
            r = jnp.dot(act[...], proj[:, ks], preferred_element_type=F32).astype(BF)
            for b in range(4):
                part[b, 0:block, ks] = r[b * block : (b + 1) * block, :]

        tiles(wide // 512, 512, outer)

    wing = wide // 2
    right, left, across = column(1), column(3), column(2)

    piece = block // 2

    def reduce_copy(n):
        if n < 2:
            source = part.at[across, :, pl.ds(n * wing, wing)]
            target = first.at[n]
        else:
            span = pl.ds((n // 2 - 1) * piece, piece)
            source = part.at[right if n % 2 == 0 else left, span]
            target = second.at[n % 2, span]
        return pltpu.make_async_remote_copy(
            src_ref=source,
            dst_ref=target,
            send_sem=qs.at[n],
            recv_sem=qr.at[n],
            device_id={"tp": right if n % 2 == 0 else left},
            device_id_type=MESH,
        )

    def reduce_start():
        reduce_copy(0).start()
        reduce_copy(1).start()

    def reduce_pass(q):
        if q == 0:
            reduce_copy(0).wait_recv()
            reduce_copy(1).wait_recv()
        span = pl.ds(q * piece, piece)
        for n, owner in ((0, right), (1, left)):
            for k in range(wing // 512):
                cols = slice(n * wing + 512 * k, n * wing + 512 * k + 512)
                part[owner, span, cols] = (
                    part[owner, span, cols].astype(F32)
                    + first[n, span, 512 * k : 512 * k + 512].astype(F32)
                ).astype(BF)
            reduce_copy(2 * q + 2 + n).start()

    def reduce_end():
        for n in range(2, 10):
            reduce_copy(n).wait_recv()

        def body(ks):
            second[0, :, ks] = (
                part[t, :, ks].astype(F32)
                + second[0, :, ks].astype(F32)
                + second[1, :, ks].astype(F32)
            ).astype(BF)

        tiles(wide // 512, 512, body)
        for copy in result:
            copy.start()

    result = [
        pltpu.make_async_copy(second.at[0, pl.ds(0, block)], mixer_out, sem_local.at[10]),
        pltpu.make_async_copy(second.at[0, pl.ds(block, block)], shared_out, sem_local.at[11]),
    ]

    def receive(g):
        for i in range(8 * g, 8 * g + 8):
            if i == 0:
                own_rows.wait()
            else:
                arrival(i).wait_recv()
            forward(i).start()

    def hidden(g):
        for i in range(8 * g, 8 * g + 8):
            forward(i).wait_recv()
        span = pl.ds(g * group, group)
        acc[...] = jnp.zeros_like(acc)

        def body(ks):
            x = inbox[span, ks]
            acc[0:group, 0:units] += jnp.dot(x, gate[ks, :], preferred_element_type=F32)
            acc[0:group, units : 2 * units] += jnp.dot(x, up[ks, :], preferred_element_type=F32)

        tiles(depth // 1024, 1024, body)
        a = acc[0:group, 0:units]
        hid[span, features(t, units)] = (
            a * (1.0 / (1.0 + jnp.exp(-a))) * acc[0:group, units : 2 * units]
        ).astype(BF)
        hidden_copy(g, 1).start()
        hidden_copy(g, 3).start()

    def pass_hidden(g):
        hidden_copy(g, 1).wait_recv()
        hidden_copy(g, 3).wait_recv()
        hidden_copy(g, 2).start()

    def project(g):
        hidden_copy(g, 2).wait_recv()
        span = pl.ds(g * group, group)
        step = 256

        def body(k, carry):
            ks = pl.ds(pl.multiple_of(k * step, step), step)
            outs[span, ks] = jnp.dot(
                hid[span, :], wdn[:, ks], preferred_element_type=F32
            ).astype(BF)
            return carry

        lax.fori_loop(0, width // step, body, 0)
        for n in range(4 * g, 4 * g + 4):
            if n in TURNS:
                back_to_corner(n).start()
            else:
                if n == 0:
                    own_back.start()
                else:
                    give_back(2 * n).start()
                give_back(2 * n + 1).start()

    def turn(ks_):
        for k in ks_:
            to_corner(TURNS[k]).wait_recv()
            from_corner(2 * TURNS[k]).start()
            from_corner(2 * TURNS[k] + 1).start()

    def turn_back(g):
        for n in range(4 * g, 4 * g + 4):
            if n in TURNS:
                back_to_corner(n).wait_recv()
                back_from_corner(2 * n).start()
                back_from_corner(2 * n + 1).start()

    shared_expert()
    turn(range(0, 2))
    convolve()
    turn(range(2, 4))
    receive(0)
    activate()
    turn(range(4, 6))
    mix()
    turn(range(6, 9))
    reduce_start()
    receive(1)
    loads[5].wait()
    loads[6].wait()
    hidden(0)
    receive(2)
    pass_hidden(0)
    hidden(1)
    own_weight.wait()
    for j in range(1, 4):
        weight_copy(j).wait()
    reduce_pass(0)
    project(0)
    receive(3)
    pass_hidden(1)
    hidden(2)
    reduce_pass(1)
    project(1)
    pass_hidden(2)
    hidden(3)
    turn_back(1)
    project(2)
    pass_hidden(3)
    reduce_pass(2)
    project(3)
    reduce_pass(3)
    turn_back(2)
    turn_back(3)
    reduce_end()

    rim_copy.wait_send()
    for j in range(1, 4):
        stats_copy(j).wait_send()
    for n in range(10):
        reduce_copy(n).wait_send()
    for copy in result:
        copy.wait()
    for i in range(1, 32):
        arrival(i).wait_send()
    for n in TURNS:
        to_corner(n).wait_send()
        back_to_corner(n).wait_send()
    for i in range(32):
        forward(i).wait_send()
    for g in range(4):
        for j in range(1, 4):
            hidden_copy(g, j).wait_send()
    own_back.wait()
    for i in range(1, 32):
        return_leg(i).wait()


def routed_rows(outbox, normed, mixer, weights):
    count, rows, sent = outbox.shape
    depth, units = weights[0].shape
    width = weights[2].shape[1] // 4
    total = count * rows
    length, channels = mixer[0].shape
    wide = weights[2].shape[1]
    block = length // 4
    dma = pltpu.SemaphoreType.DMA
    vmem = pl.BlockSpec(memory_space=pltpu.VMEM)
    hbm = pl.BlockSpec(memory_space=pl.ANY)
    return pl.pallas_call(
        expert_kernel,
        out_shape=(
            jax.ShapeDtypeStruct((count, rows, width), BF),
            jax.ShapeDtypeStruct((block, wide), BF),
            jax.ShapeDtypeStruct((block, wide), BF),
            jax.ShapeDtypeStruct((len(TURNS), 2, rows, sent), BF),
            jax.ShapeDtypeStruct((len(TURNS), 2 * rows, width), BF),
        ),
        in_specs=[hbm, hbm] + [vmem] * 6 + [hbm] * 7,
        out_specs=(hbm,) * 5,
        scratch_shapes=[
            pltpu.VMEM((total, depth), BF),
            pltpu.VMEM((total, 4 * units), BF),
            pltpu.VMEM((4 * units, width), BF),
            pltpu.VMEM((total, width), BF),
            pltpu.VMEM((length, 2 * units), F32),
            pltpu.VMEM((depth, units), BF),
            pltpu.VMEM((depth, units), BF),
            pltpu.VMEM((length + 32, channels), F32),
            pltpu.VMEM((length, channels), F32),
            pltpu.VMEM((length, channels), BF),
            pltpu.VMEM((32, channels), BF),
            pltpu.VMEM((32, channels), BF),
            pltpu.VMEM((4, 8, length), F32),
            pltpu.VMEM((channels, wide), BF),
            pltpu.VMEM((length, wide), BF),
            pltpu.VMEM((depth, units), BF),
            pltpu.VMEM((depth, units), BF),
            pltpu.VMEM((units, wide), BF),
            pltpu.VMEM((length, units), BF),
            pltpu.VMEM((4, 2 * block, wide), BF),
            pltpu.VMEM((2, 2 * block, wide // 2), BF),
            pltpu.VMEM((2, 2 * block, wide), BF),
            dma((12,)),
            dma((1,)),
            dma((1,)),
            dma((4,)),
            dma((4,)),
            dma((10,)),
            dma((10,)),
            dma((32,)),
            dma((32,)),
            dma((32,)),
            dma((32,)),
            dma((4, 4)),
            dma((4, 4)),
            dma((4,)),
            dma((4,)),
            dma((32,)),
            dma((32,)),
            dma((9,)),
            dma((9,)),
            dma((9,)),
            dma((9,)),
        ],
        compiler_params=pltpu.CompilerParams(
            collective_id=0, has_side_effects=True, vmem_limit_bytes=67_043_328
        ),
    )(outbox, normed, *mixer, *weights)


def per_device(
    value_in,
    gate_in,
    conv_taps,
    conv_bias,
    ln_gain,
    ln_bias,
    out_proj,
    tokens_b,
    norm_gain,
    routes,
    route_weights,
    expert_gate,
    expert_up,
    expert_down,
    shared_gate,
    shared_up,
    shared_down,
):
    tp_count = lax.axis_size("tp")
    ep_count = lax.axis_size("ep")
    t = lax.axis_index("tp")
    rows_own, top_count = routes.shape
    rows_all = rows_own * tp_count
    model_width = tokens_b.shape[1]

    tables = lax.all_gather(
        jnp.concatenate([routes.astype(F32), route_weights], axis=1), "tp", axis=0
    )
    chosen = tables[:, :, :top_count].astype(jnp.int32).reshape(tp_count, -1)
    weights = tables[:, :, top_count:].reshape(rows_all, top_count)
    onehot = (chosen[:, :, None] == jnp.arange(ep_count, dtype=jnp.int32)).astype(BF)
    pairs = chosen.shape[1]
    lower = (
        jnp.arange(pairs, dtype=jnp.int32)[:, None] > jnp.arange(pairs, dtype=jnp.int32)[None, :]
    ).astype(BF)
    earlier = jnp.einsum("ij,bje->bie", lower, onehot, preferred_element_type=F32)
    places = jnp.sum(earlier * onehot.astype(F32), axis=2).astype(jnp.int32)
    slots = (
        chosen * (tp_count * CAP)
        + jnp.arange(tp_count, dtype=jnp.int32)[:, None] * CAP
        + places
    ).reshape(rows_all, top_count)
    slot_count = ep_count * tp_count * CAP

    features = tokens_b.astype(F32)
    normed_b = (
        features
        * lax.rsqrt(jnp.mean(features * features, axis=1, keepdims=True) + EPSILON)
        * norm_gain
    ).astype(BF)
    sent = model_width - EDGE
    part = lax.dynamic_slice_in_dim(normed_b, (1 - t % 2) * EDGE, sent, 1)
    ids = jnp.arange(slot_count, dtype=jnp.int32)
    select = (
        (ids[:, None] == slots[None, :, 0]) | (ids[:, None] == slots[None, :, 1])
    ).astype(BF)
    outbox = jnp.dot(select, part, preferred_element_type=F32).astype(BF)
    outbox = outbox.reshape(ep_count, tp_count * CAP, sent)

    returned, mixer_rows, shared_rows, _, _ = routed_rows(
        outbox,
        normed_b,
        (
            value_in,
            gate_in,
            conv_taps,
            conv_bias[None, :],
            ln_gain[None, :],
            ln_bias[None, :],
            out_proj,
        ),
        (
            expert_gate[0],
            expert_up[0],
            expert_down[0],
            shared_gate,
            shared_up,
            shared_down,
        ),
    )
    returned = returned.reshape(slot_count, -1)
    spread = jnp.where(ids[None, :] == slots[:, 0:1], weights[:, 0:1], 0.0) + jnp.where(
        ids[None, :] == slots[:, 1:2], weights[:, 1:2], 0.0
    )
    high = spread.astype(BF)
    low = (spread - high.astype(F32)).astype(BF)
    combined = jnp.dot(high, returned, preferred_element_type=F32) + jnp.dot(
        low, returned, preferred_element_type=F32
    )
    quarters = lax.all_to_all(
        combined.astype(BF).reshape(tp_count, rows_own, -1), "tp", 0, 0, tiled=True
    )
    routed = jnp.moveaxis(quarters, 0, 1).reshape(rows_own, model_width)
    experts_out = (shared_rows.astype(F32) + routed.astype(F32)).astype(BF)
    return (mixer_rows, experts_out)


def solution(mesh):
    return jax.shard_map(
        per_device,
        mesh=mesh,
        in_specs=(
            P("ep", "tp"),
            P("ep", "tp"),
            P(None, "tp"),
            P("tp"),
            P("tp"),
            P("tp"),
            P("tp", None),
            P("ep", None),
            P(),
            P(("ep", "tp"), None),
            P(("ep", "tp"), None),
            P("ep", None, "tp"),
            P("ep", None, "tp"),
            P("ep", "tp", None),
            P(None, "tp"),
            P(None, "tp"),
            P("tp", None),
        ),
        out_specs=(P(("ep", "tp"), None), P(("ep", "tp"), None)),
        check_vma=False,
    )
```

```python
import functools

import jax
import jax.numpy as jnp
from jax import lax
from jax.experimental import pallas as pl
from jax.experimental.pallas import tpu as pltpu
from jax.sharding import PartitionSpec as P

EPSILON = 1e-06
MESH = pl.DeviceIdType.MESH
CAP = 12
EDGE = 1024
PAIRS = [
    (0, 0), (0, 1), (1, 0), (0, 3),
    (3, 0), (1, 1), (3, 1), (0, 2),
    (2, 0), (2, 1), (1, 3), (3, 3),
    (2, 3), (1, 2), (3, 2), (2, 2),
]
TURNS = [n for n, (a, b) in enumerate(PAIRS) if a and b]
STRAIGHT = [n for n, (a, b) in enumerate(PAIRS) if (a or b) and not (a and b)]
BF = jnp.bfloat16
F32 = jnp.float32


def expert_kernel(
    outbox,
    normed,
    value_in,
    gate_in,
    taps,
    conv_bias,
    ln_gain,
    ln_bias,
    proj_in,
    gate_hbm,
    up_hbm,
    down,
    sgate_hbm,
    sup_hbm,
    sdown_hbm,
    spread,
    mixer_out,
    experts_out,
    corner,
    corner_back,
    inbox,
    hid,
    wdn,
    outs,
    acc,
    gate,
    up,
    padded,
    filt,
    act,
    rim,
    rim_out,
    stats,
    proj,
    nb,
    sgate,
    sup,
    sdown,
    shid,
    part,
    first,
    second,
    ret,
    sem_local,
    xs,
    xr,
    cs,
    cr,
    ss,
    sr,
    qs,
    qr,
    ds,
    dr,
    fs,
    fr,
    hs,
    hr,
    ws,
    wr,
    rs,
    rr,
    ks,
    kr,
    bs,
    br,
):
    me = lax.axis_index("ep")
    t = lax.axis_index("tp")
    z, y, c = me // 8, (me // 2) % 4, me % 2
    p = t % 2
    rows = outbox.shape[1]
    sent = outbox.shape[2]
    rest = gate.shape[0] - sent
    mine = pl.ds(pl.multiple_of((1 - p) * rest, 128), sent)
    lacking = pl.ds(pl.multiple_of((1 - p) * sent, 128), rest)
    group = 8 * rows
    units = gate.shape[1]
    width = wdn.shape[1]
    depth = gate.shape[0]

    def away(dz, dy, dc):
        return ((z + 4 + dz) % 4) * 8 + ((y + 4 + dy) % 4) * 2 + (c + dc) % 2

    def ahead(i):
        dz, dy = PAIRS[i // 2]
        return away(dz, dy, i % 2)

    def behind(i):
        dz, dy = PAIRS[i // 2]
        return away(-dz, -dy, i % 2)

    def legs(n):
        dz, dy = PAIRS[n]
        return ((0, dy), (dz, 0)) if (dz + dy) % 2 == 0 else ((dz, 0), (0, dy))

    def column(j):
        return (t + j) % 4

    def features(q, size):
        return pl.ds(pl.multiple_of(q * size, size), size)

    loads = [
        pltpu.make_async_copy(a, b, sem_local.at[3 + n])
        for n, (a, b) in enumerate(
            [
                (normed, nb),
                (sgate_hbm, sgate),
                (sup_hbm, sup),
                (sdown_hbm, sdown),
                (proj_in, proj),
                (gate_hbm, gate),
                (up_hbm, up),
            ]
        )
    ]
    barrier = pltpu.get_barrier_semaphore()
    for i in range(1, 32):
        pl.semaphore_signal(barrier, inc=1, device_id={"ep": ahead(i)}, device_id_type=MESH)
    for j in range(1, 4):
        pl.semaphore_signal(barrier, inc=1, device_id={"tp": column(j)}, device_id_type=MESH)
    pl.semaphore_wait(barrier, 34)

    def weight_copy(j):
        return pltpu.make_async_remote_copy(
            src_ref=down.at[:, features(column(j), width)],
            dst_ref=wdn.at[features(t, units), :],
            send_sem=ws.at[j],
            recv_sem=wr.at[j],
            device_id={"tp": column(j)},
            device_id_type=MESH,
        )

    own_weight = pltpu.make_async_copy(
        down.at[:, features(t, width)], wdn.at[features(t, units), :], sem_local.at[0]
    )
    own_rows = pltpu.make_async_copy(
        outbox.at[me], inbox.at[pl.ds(0, rows), mine], sem_local.at[1]
    )

    def dispatch(i):
        return pltpu.make_async_remote_copy(
            src_ref=outbox.at[ahead(i)],
            dst_ref=inbox.at[pl.ds(i * rows, rows), mine],
            send_sem=ds.at[i],
            recv_sem=dr.at[i],
            device_id={"ep": ahead(i)},
            device_id_type=MESH,
        )

    def to_corner(n):
        dz, dy = PAIRS[n]
        start = ((z + dz) % 4) * 8 + ((y + dy) % 4) * 2
        k = TURNS.index(n)
        leg = legs(n)[0]
        return pltpu.make_async_remote_copy(
            src_ref=outbox.at[pl.ds(start, 2)],
            dst_ref=corner.at[k],
            send_sem=ks.at[k],
            recv_sem=kr.at[k],
            device_id={"ep": away(*leg, 0)},
            device_id_type=MESH,
        )

    def from_corner(i):
        k = TURNS.index(i // 2)
        leg = legs(i // 2)[1]
        return pltpu.make_async_remote_copy(
            src_ref=corner.at[k, (c + i % 2) % 2],
            dst_ref=inbox.at[pl.ds(i * rows, rows), mine],
            send_sem=ds.at[i],
            recv_sem=dr.at[i],
            device_id={"ep": away(*leg, i % 2)},
            device_id_type=MESH,
        )

    def arrival(i):
        return from_corner(i) if i // 2 in TURNS else dispatch(i)

    def back_to_corner(n):
        k = TURNS.index(n)
        leg = legs(n)[0]
        return pltpu.make_async_remote_copy(
            src_ref=outs.at[pl.ds(n * 2 * rows, 2 * rows), :],
            dst_ref=corner_back.at[k],
            send_sem=bs.at[k],
            recv_sem=br.at[k],
            device_id={"ep": away(-leg[0], -leg[1], 0)},
            device_id_type=MESH,
        )

    def back_from_corner(i):
        k = TURNS.index(i // 2)
        one, two = legs(i // 2)
        return pltpu.make_async_remote_copy(
            src_ref=corner_back.at[k, pl.ds((i % 2) * rows, rows)],
            dst_ref=ret.at[away(*one, 0)],
            send_sem=rs.at[i],
            recv_sem=rr.at[i],
            device_id={"ep": away(-two[0], -two[1], i % 2)},
            device_id_type=MESH,
        )

    def return_leg(i):
        return back_from_corner(i) if i // 2 in TURNS else give_back(i)

    def forward(i):
        place = inbox.at[pl.ds(i * rows, rows), lacking]
        return pltpu.make_async_remote_copy(
            src_ref=place,
            dst_ref=place,
            send_sem=fs.at[i],
            recv_sem=fr.at[i],
            device_id={"tp": column(1 if i % 2 == 0 else 3)},
            device_id_type=MESH,
        )

    def hidden_copy(g, j):
        to = j
        source = t
        if j == 2:
            to = 1 if g % 2 == 0 else 3
            source = column(4 - to)
        place = hid.at[pl.ds(g * group, group), features(source, units)]
        return pltpu.make_async_remote_copy(
            src_ref=place,
            dst_ref=place,
            send_sem=hs.at[g, j],
            recv_sem=hr.at[g, j],
            device_id={"tp": column(to)},
            device_id_type=MESH,
        )

    def give_back(i):
        return pltpu.make_async_remote_copy(
            src_ref=outs.at[pl.ds(i * rows, rows), :],
            dst_ref=ret.at[me],
            send_sem=rs.at[i],
            recv_sem=rr.at[i],
            device_id={"ep": behind(i)},
            device_id_type=MESH,
        )

    own_back = pltpu.make_async_copy(outs.at[pl.ds(0, rows), :], ret.at[me], sem_local.at[2])

    own_rows.start()
    dispatch(1).start()
    straight = list(STRAIGHT)
    for count, n in enumerate(TURNS):
        to_corner(n).start()
        if count % 3 == 0:
            for _ in range(2):
                m = straight.pop(0)
                dispatch(2 * m).start()
                dispatch(2 * m + 1).start()
    own_weight.start()
    for j in range(1, 4):
        weight_copy(j).start()
    for load in loads:
        load.start()

    length, channels = value_in.shape
    edge = rim.shape[0]
    tap_count = taps.shape[0]
    block = length // 4
    wide = nb.shape[1]

    rim_copy = pltpu.make_async_remote_copy(
        src_ref=rim_out,
        dst_ref=rim,
        send_sem=cs.at[0],
        recv_sem=cr.at[0],
        device_id={"ep": (me + 1) % 32},
        device_id_type=MESH,
    )

    def stats_copy(j):
        return pltpu.make_async_remote_copy(
            src_ref=stats.at[t],
            dst_ref=stats.at[t],
            send_sem=ss.at[j],
            recv_sem=sr.at[j],
            device_id={"tp": column(j)},
            device_id_type=MESH,
        )

    def tiles(count, size, body):
        def step(k, carry):
            body(pl.ds(pl.multiple_of(k * size, size), size))
            return carry

        lax.fori_loop(0, count, step, 0)

    def gated_tile(span):
        g = gate_in[span, :].astype(F32)
        v = value_in[span, :].astype(F32) * (1.0 / (1.0 + jnp.exp(-g)))
        padded[pl.ds(pl.multiple_of(span.start + edge, edge), 64), :] = v.astype(BF).astype(F32)

    tiles(length // 64, 64, gated_tile)
    rim_out[...] = padded[length : length + edge, :].astype(BF)
    rim_copy.start()

    def shared_expert():
        for load in loads[:4]:
            load.wait()
        acc[...] = jnp.zeros_like(acc)

        def inner(ks):
            x = nb[:, ks]
            acc[:, 0:units] += jnp.dot(x, sgate[ks, :], preferred_element_type=F32)
            acc[:, units : 2 * units] += jnp.dot(x, sup[ks, :], preferred_element_type=F32)

        tiles(depth // 1024, 1024, inner)
        a = acc[:, 0:units]
        shid[...] = (a * (1.0 / (1.0 + jnp.exp(-a))) * acc[:, units : 2 * units]).astype(BF)

        def outer(ks):
            r = jnp.dot(shid[...], sdown[:, ks], preferred_element_type=F32).astype(BF)
            for b in range(4):
                part[b, block : 2 * block, ks] = r[b * block : (b + 1) * block, :]

        tiles(wide // 512, 512, outer)

    def convolve():
        rim_copy.wait_recv()
        padded[0:edge, :] = jnp.where(me == 0, 0.0, rim[...].astype(F32))

        def strip(k, carry):
            for q in range(channels // 128):
                cols = slice(128 * q, 128 * q + 128)
                window = padded[pl.ds(pl.multiple_of(k * 64, 64), 64 + edge), cols]
                total = jnp.zeros((64, 128), F32) + conv_bias[:, cols]
                for rest in range(8):
                    turned = window[rest : rest + 56 + edge, :] if rest else window
                    for tap in range(tap_count):
                        at = edge + 1 - tap_count + tap
                        if at % 8 == rest:
                            base = at - rest
                            total = total + taps[tap : tap + 1, cols] * turned[base : base + 64, :]
                filt[pl.ds(pl.multiple_of(k * 64, 64), 64), cols] = total
            return carry

        lax.fori_loop(0, length // 64, strip, 0)
        lane = lax.broadcasted_iota(jnp.int32, (128, 128), 1)
        for b in range(length // 128):
            rs_ = slice(128 * b, 128 * b + 128)
            f = filt[rs_, :]
            both = jnp.where(
                lane == 0,
                jnp.sum(f, axis=1, keepdims=True),
                jnp.where(lane == 1, jnp.sum(f * f, axis=1, keepdims=True), 0.0),
            )
            stats[t, :, rs_] = both.T[0:8, :]
        for j in range(1, 4):
            stats_copy(j).start()

    def activate():
        for j in range(1, 4):
            stats_copy(j).wait_recv()
        whole = 4.0 * channels
        for b in range(length // 128):
            rs_ = slice(128 * b, 128 * b + 128)
            total = (stats[0, :, rs_] + stats[1, :, rs_]) + (stats[2, :, rs_] + stats[3, :, rs_])
            turned = jnp.concatenate([total, jnp.zeros((120, 128), F32)], axis=0).T
            average = turned[:, 0:1] / whole
            variance = turned[:, 1:2] / whole - average * average
            v = (filt[rs_, :] - average) * lax.rsqrt(variance + EPSILON) * ln_gain[...] + ln_bias[
                ...
            ]
            act[rs_, :] = (v / (1.0 + jnp.exp(-v))).astype(BF)

    def mix():
        loads[4].wait()

        def outer(ks):
            r = jnp.dot(act[...], proj[:, ks], preferred_element_type=F32).astype(BF)
            for b in range(4):
                part[b, 0:block, ks] = r[b * block : (b + 1) * block, :]

        tiles(wide // 512, 512, outer)

    wing = wide // 2
    right, left, across = column(1), column(3), column(2)

    piece = block // 2

    def reduce_copy(n):
        if n < 2:
            source = part.at[across, :, pl.ds(n * wing, wing)]
            target = first.at[n]
        else:
            span = pl.ds((n // 2 - 1) * piece, piece)
            source = part.at[right if n % 2 == 0 else left, span]
            target = second.at[n % 2, span]
        return pltpu.make_async_remote_copy(
            src_ref=source,
            dst_ref=target,
            send_sem=qs.at[n],
            recv_sem=qr.at[n],
            device_id={"tp": right if n % 2 == 0 else left},
            device_id_type=MESH,
        )

    def reduce_start():
        reduce_copy(0).start()
        reduce_copy(1).start()

    def reduce_pass(q):
        if q == 0:
            reduce_copy(0).wait_recv()
            reduce_copy(1).wait_recv()
        span = pl.ds(q * piece, piece)
        for n, owner in ((0, right), (1, left)):
            for k in range(wing // 512):
                cols = slice(n * wing + 512 * k, n * wing + 512 * k + 512)
                part[owner, span, cols] = (
                    part[owner, span, cols].astype(F32)
                    + first[n, span, 512 * k : 512 * k + 512].astype(F32)
                ).astype(BF)
            reduce_copy(2 * q + 2 + n).start()

    def reduce_end():
        for n in range(2, 10):
            reduce_copy(n).wait_recv()

        def body(ks):
            second[0, :, ks] = (
                part[t, :, ks].astype(F32)
                + second[0, :, ks].astype(F32)
                + second[1, :, ks].astype(F32)
            ).astype(BF)

        tiles(wide // 512, 512, body)
        result[0].start()

    result = [
        pltpu.make_async_copy(second.at[0, pl.ds(0, block)], mixer_out, sem_local.at[10]),
        pltpu.make_async_copy(sdown.at[pl.ds(0, block)], experts_out, sem_local.at[11]),
    ]

    load_spread = pltpu.make_async_copy(
        spread, proj.at[:, pl.ds(0, spread.shape[1])], sem_local.at[12]
    )

    def quarter_copy(j):
        return pltpu.make_async_remote_copy(
            src_ref=nb.at[pl.ds(pl.multiple_of(column(j) * block, block), block), pl.ds(0, width)],
            dst_ref=sdown.at[pl.ds(0, block), features(t, width)],
            send_sem=xs.at[j],
            recv_sem=xr.at[j],
            device_id={"tp": column(j)},
            device_id_type=MESH,
        )

    def combine(j):
        span = pl.ds(pl.multiple_of(column(j) * block, block), block)
        slots = hid.shape[0]
        for k in range(2):
            cols = slice(k * width // 2, (k + 1) * width // 2)
            values = ret[:, :, cols].reshape(slots, width // 2)
            total = jnp.dot(
                proj[span, 0:slots], values, preferred_element_type=F32
            ) + jnp.dot(proj[span, slots : 2 * slots], values, preferred_element_type=F32)
            nb[span, cols] = total.astype(BF)

    def finish():
        for j in (2, 1, 3):
            combine(j)
            quarter_copy(j).start()
        combine(0)
        own = nb[pl.ds(pl.multiple_of(t * block, block), block), 0:width]
        sdown[0:block, features(t, width)] = own

    def last_sum():
        for j in range(1, 4):
            quarter_copy(j).wait_recv()

        def body(cols):
            sdown[0:block, cols] = (
                second[0, block : 2 * block, cols].astype(F32) + sdown[0:block, cols].astype(F32)
            ).astype(BF)

        tiles(wide // 512, 512, body)
        result[1].start()

    def receive(g):
        for i in range(8 * g, 8 * g + 8):
            if i == 0:
                own_rows.wait()
            else:
                arrival(i).wait_recv()
            forward(i).start()

    def hidden(g):
        for i in range(8 * g, 8 * g + 8):
            forward(i).wait_recv()
        span = pl.ds(g * group, group)
        acc[...] = jnp.zeros_like(acc)

        def body(ks):
            x = inbox[span, ks]
            acc[0:group, 0:units] += jnp.dot(x, gate[ks, :], preferred_element_type=F32)
            acc[0:group, units : 2 * units] += jnp.dot(x, up[ks, :], preferred_element_type=F32)

        tiles(depth // 1024, 1024, body)
        a = acc[0:group, 0:units]
        hid[span, features(t, units)] = (
            a * (1.0 / (1.0 + jnp.exp(-a))) * acc[0:group, units : 2 * units]
        ).astype(BF)
        hidden_copy(g, 1).start()
        hidden_copy(g, 3).start()

    def pass_hidden(g):
        hidden_copy(g, 1).wait_recv()
        hidden_copy(g, 3).wait_recv()
        hidden_copy(g, 2).start()

    def project(g):
        hidden_copy(g, 2).wait_recv()
        span = pl.ds(g * group, group)
        step = 256

        def body(k, carry):
            ks = pl.ds(pl.multiple_of(k * step, step), step)
            outs[span, ks] = jnp.dot(
                hid[span, :], wdn[:, ks], preferred_element_type=F32
            ).astype(BF)
            return carry

        lax.fori_loop(0, width // step, body, 0)
        for n in range(4 * g, 4 * g + 4):
            if n in TURNS:
                back_to_corner(n).start()
            else:
                if n == 0:
                    own_back.start()
                else:
                    give_back(2 * n).start()
                give_back(2 * n + 1).start()

    def turn(ks_):
        for k in ks_:
            to_corner(TURNS[k]).wait_recv()
            from_corner(2 * TURNS[k]).start()
            from_corner(2 * TURNS[k] + 1).start()

    def turn_back(g):
        for n in range(4 * g, 4 * g + 4):
            if n in TURNS:
                back_to_corner(n).wait_recv()
                back_from_corner(2 * n).start()
                back_from_corner(2 * n + 1).start()

    shared_expert()
    turn(range(0, 2))
    convolve()
    turn(range(2, 4))
    receive(0)
    activate()
    turn(range(4, 6))
    mix()
    load_spread.start()
    turn(range(6, 9))
    reduce_start()
    receive(1)
    loads[5].wait()
    loads[6].wait()
    hidden(0)
    receive(2)
    pass_hidden(0)
    hidden(1)
    own_weight.wait()
    for j in range(1, 4):
        weight_copy(j).wait()
    reduce_pass(0)
    project(0)
    receive(3)
    pass_hidden(1)
    hidden(2)
    reduce_pass(1)
    project(1)
    pass_hidden(2)
    hidden(3)
    turn_back(1)
    project(2)
    pass_hidden(3)
    reduce_pass(2)
    project(3)
    reduce_pass(3)
    turn_back(2)
    turn_back(3)
    own_back.wait()
    for i in range(1, 32):
        return_leg(i).wait_recv()
    load_spread.wait()
    finish()
    reduce_end()
    last_sum()

    rim_copy.wait_send()
    for j in range(1, 4):
        stats_copy(j).wait_send()
    for n in range(10):
        reduce_copy(n).wait_send()
    result[0].wait()
    for i in range(1, 32):
        arrival(i).wait_send()
    for n in TURNS:
        to_corner(n).wait_send()
        back_to_corner(n).wait_send()
    for i in range(32):
        forward(i).wait_send()
    for g in range(4):
        for j in range(1, 4):
            hidden_copy(g, j).wait_send()
    for i in range(1, 32):
        return_leg(i).wait_send()
    for j in range(1, 4):
        quarter_copy(j).wait_send()
    result[1].wait()


def norm_kernel(table, tokens, gain, tables, normed, sends, receives):
    t = lax.axis_index("tp")
    barrier = pltpu.get_barrier_semaphore()
    for j in range(1, 4):
        pl.semaphore_signal(barrier, inc=1, device_id={"tp": (t + j) % 4}, device_id_type=MESH)
    pl.semaphore_wait(barrier, 3)

    def table_copy(j):
        return pltpu.make_async_remote_copy(
            src_ref=table,
            dst_ref=tables.at[t],
            send_sem=sends.at[j],
            recv_sem=receives.at[j],
            device_id={"tp": (t + j) % 4},
            device_id_type=MESH,
        )

    for j in range(1, 4):
        table_copy(j).start()
    tables[t] = table[...]
    size = 32

    def body(k, carry):
        span = pl.ds(pl.multiple_of(k * size, size), size)
        x = tokens[span, :].astype(F32)
        scale = lax.rsqrt(jnp.mean(x * x, axis=1, keepdims=True) + EPSILON)
        normed[span, :] = (x * scale * gain[...]).astype(BF)
        return carry

    lax.fori_loop(0, tokens.shape[0] // size, body, 0)
    for j in range(1, 4):
        table_copy(j).wait()


def normed_rows(table, tokens, gain):
    vmem = pl.BlockSpec(memory_space=pltpu.VMEM)
    return pl.pallas_call(
        norm_kernel,
        out_shape=(
            jax.ShapeDtypeStruct((4, *table.shape), F32),
            jax.ShapeDtypeStruct(tokens.shape, BF),
        ),
        in_specs=[vmem] * 3,
        out_specs=(vmem, vmem),
        scratch_shapes=[pltpu.SemaphoreType.DMA((4,)), pltpu.SemaphoreType.DMA((4,))],
        compiler_params=pltpu.CompilerParams(
            collective_id=1, has_side_effects=True, vmem_limit_bytes=24 * 1024 * 1024
        ),
    )(table, tokens, gain[None, :])


def routed_rows(outbox, normed, mixer, weights, spread):
    count, rows, sent = outbox.shape
    depth, units = weights[0].shape
    width = weights[2].shape[1] // 4
    total = count * rows
    length, channels = mixer[0].shape
    wide = weights[2].shape[1]
    block = length // 4
    dma = pltpu.SemaphoreType.DMA
    vmem = pl.BlockSpec(memory_space=pltpu.VMEM)
    hbm = pl.BlockSpec(memory_space=pl.ANY)
    return pl.pallas_call(
        expert_kernel,
        out_shape=(
            jax.ShapeDtypeStruct((block, wide), BF),
            jax.ShapeDtypeStruct((block, wide), BF),
            jax.ShapeDtypeStruct((len(TURNS), 2, rows, sent), BF),
            jax.ShapeDtypeStruct((len(TURNS), 2 * rows, width), BF),
        ),
        in_specs=[hbm, hbm] + [vmem] * 6 + [hbm] * 8,
        out_specs=(hbm,) * 4,
        scratch_shapes=[
            pltpu.VMEM((total, depth), BF),
            pltpu.VMEM((total, 4 * units), BF),
            pltpu.VMEM((4 * units, width), BF),
            pltpu.VMEM((total, width), BF),
            pltpu.VMEM((length, 2 * units), F32),
            pltpu.VMEM((depth, units), BF),
            pltpu.VMEM((depth, units), BF),
            pltpu.VMEM((length + 32, channels), F32),
            pltpu.VMEM((length, channels), F32),
            pltpu.VMEM((length, channels), BF),
            pltpu.VMEM((32, channels), BF),
            pltpu.VMEM((32, channels), BF),
            pltpu.VMEM((4, 8, length), F32),
            pltpu.VMEM((channels, wide), BF),
            pltpu.VMEM((length, wide), BF),
            pltpu.VMEM((depth, units), BF),
            pltpu.VMEM((depth, units), BF),
            pltpu.VMEM((units, wide), BF),
            pltpu.VMEM((length, units), BF),
            pltpu.VMEM((4, 2 * block, wide), BF),
            pltpu.VMEM((2, 2 * block, wide // 2), BF),
            pltpu.VMEM((2, 2 * block, wide), BF),
            pltpu.VMEM((count, rows, width), BF),
            dma((13,)),
            dma((4,)),
            dma((4,)),
            dma((1,)),
            dma((1,)),
            dma((4,)),
            dma((4,)),
            dma((10,)),
            dma((10,)),
            dma((32,)),
            dma((32,)),
            dma((32,)),
            dma((32,)),
            dma((4, 4)),
            dma((4, 4)),
            dma((4,)),
            dma((4,)),
            dma((32,)),
            dma((32,)),
            dma((9,)),
            dma((9,)),
            dma((9,)),
            dma((9,)),
        ],
        compiler_params=pltpu.CompilerParams(
            collective_id=0, has_side_effects=True, vmem_limit_bytes=67_043_328
        ),
    )(outbox, normed, *mixer, *weights, spread)


def per_device(
    value_in,
    gate_in,
    conv_taps,
    conv_bias,
    ln_gain,
    ln_bias,
    out_proj,
    tokens_b,
    norm_gain,
    routes,
    route_weights,
    expert_gate,
    expert_up,
    expert_down,
    shared_gate,
    shared_up,
    shared_down,
):
    tp_count = lax.axis_size("tp")
    ep_count = lax.axis_size("ep")
    t = lax.axis_index("tp")
    rows_own, top_count = routes.shape
    rows_all = rows_own * tp_count
    model_width = tokens_b.shape[1]

    own = jnp.concatenate(
        [
            routes.astype(F32).T,
            route_weights.T,
            jnp.zeros((8 - 2 * top_count, rows_own), F32),
        ],
        axis=0,
    )
    tables, normed_b = normed_rows(own, tokens_b, norm_gain)
    chosen = jnp.swapaxes(tables[:, 0:top_count, :], 1, 2).astype(jnp.int32)
    weights = jnp.swapaxes(tables[:, top_count : 2 * top_count, :], 1, 2)
    weights = weights.reshape(rows_all, top_count)
    onehot = chosen[:, :, :, None] == jnp.arange(ep_count, dtype=jnp.int32)
    named = jnp.sum(onehot.astype(F32), axis=2).astype(BF)
    ranks = jnp.arange(rows_own, dtype=jnp.int32)
    lower = (ranks[:, None] > ranks[None, :]).astype(BF)
    earlier = jnp.einsum("ij,bje->bie", lower, named, preferred_element_type=F32)
    places = jnp.sum(jnp.where(onehot, earlier[:, :, None, :], 0.0), axis=3).astype(jnp.int32)
    slots = (
        chosen * (tp_count * CAP)
        + jnp.arange(tp_count, dtype=jnp.int32)[:, None, None] * CAP
        + places
    ).reshape(rows_all, top_count)
    slot_count = ep_count * tp_count * CAP

    sent = model_width - EDGE
    part = lax.dynamic_slice_in_dim(normed_b, (1 - t % 2) * EDGE, sent, 1)
    ids = jnp.arange(slot_count, dtype=jnp.int32)
    select = (
        (ids[:, None] == slots[None, :, 0]) | (ids[:, None] == slots[None, :, 1])
    ).astype(BF)
    outbox = jnp.dot(select, part, preferred_element_type=F32).astype(BF)
    outbox = outbox.reshape(ep_count, tp_count * CAP, sent)

    spread = jnp.where(ids[None, :] == slots[:, 0:1], weights[:, 0:1], 0.0) + jnp.where(
        ids[None, :] == slots[:, 1:2], weights[:, 1:2], 0.0
    )
    high = spread.astype(BF)
    low = (spread - high.astype(F32)).astype(BF)
    mixer_rows, expert_rows, _, _ = routed_rows(
        outbox,
        normed_b,
        (
            value_in,
            gate_in,
            conv_taps,
            conv_bias[None, :],
            ln_gain[None, :],
            ln_bias[None, :],
            out_proj,
        ),
        (
            expert_gate[0],
            expert_up[0],
            expert_down[0],
            shared_gate,
            shared_up,
            shared_down,
        ),
        jnp.concatenate([high, low], axis=1),
    )
    return (mixer_rows, expert_rows)


def solution(mesh):
    return jax.shard_map(
        per_device,
        mesh=mesh,
        in_specs=(
            P("ep", "tp"),
            P("ep", "tp"),
            P(None, "tp"),
            P("tp"),
            P("tp"),
            P("tp"),
            P("tp", None),
            P("ep", None),
            P(),
            P(("ep", "tp"), None),
            P(("ep", "tp"), None),
            P("ep", None, "tp"),
            P("ep", None, "tp"),
            P("ep", "tp", None),
            P(None, "tp"),
            P(None, "tp"),
            P("tp", None),
        ),
        out_specs=(P(("ep", "tp"), None), P(("ep", "tp"), None)),
        check_vma=False,
    )
```

```python
import functools

import jax
import jax.numpy as jnp
from jax import lax
from jax.experimental import pallas as pl
from jax.experimental.pallas import tpu as pltpu
from jax.sharding import PartitionSpec as P

EPSILON = 1e-06
MESH = pl.DeviceIdType.MESH
CAP = 12
EDGE = 1024
PAIRS = [
    (0, 0), (0, 1), (1, 0), (0, 3),
    (3, 0), (1, 1), (3, 1), (0, 2),
    (2, 0), (2, 1), (1, 3), (3, 3),
    (2, 3), (1, 2), (3, 2), (2, 2),
]
TURNS = [n for n, (a, b) in enumerate(PAIRS) if a and b]
STRAIGHT = [n for n, (a, b) in enumerate(PAIRS) if (a or b) and not (a and b)]
BF = jnp.bfloat16
F32 = jnp.float32


def expert_kernel(
    outbox,
    normed,
    value_in,
    gate_in,
    taps,
    conv_bias,
    ln_gain,
    ln_bias,
    proj_in,
    gate_hbm,
    up_hbm,
    down,
    sgate_hbm,
    sup_hbm,
    sdown_hbm,
    spread,
    mixer_out,
    experts_out,
    corner,
    corner_back,
    inbox,
    hid,
    wdn,
    outs,
    acc,
    gate,
    up,
    padded,
    filt,
    act,
    rim,
    rim_out,
    stats,
    proj,
    nb,
    sgate,
    sup,
    sdown,
    shid,
    part,
    first,
    second,
    ret,
    sem_local,
    xs,
    xr,
    cs,
    cr,
    ss,
    sr,
    qs,
    qr,
    ds,
    dr,
    fs,
    fr,
    hs,
    hr,
    ws,
    wr,
    rs,
    rr,
    ks,
    kr,
    bs,
    br,
):
    me = lax.axis_index("ep")
    t = lax.axis_index("tp")
    z, y, c = me // 8, (me // 2) % 4, me % 2
    p = t % 2
    rows = outbox.shape[1]
    sent = outbox.shape[2]
    rest = gate.shape[0] - sent
    mine = pl.ds(pl.multiple_of((1 - p) * rest, 128), sent)
    lacking = pl.ds(pl.multiple_of((1 - p) * sent, 128), rest)
    group = 8 * rows
    units = gate.shape[1]
    width = wdn.shape[1]
    depth = gate.shape[0]

    def away(dz, dy, dc):
        return ((z + 4 + dz) % 4) * 8 + ((y + 4 + dy) % 4) * 2 + (c + dc) % 2

    def ahead(i):
        dz, dy = PAIRS[i // 2]
        return away(dz, dy, i % 2)

    def behind(i):
        dz, dy = PAIRS[i // 2]
        return away(-dz, -dy, i % 2)

    def legs(n):
        dz, dy = PAIRS[n]
        return ((0, dy), (dz, 0)) if (dz + dy) % 2 == 0 else ((dz, 0), (0, dy))

    def column(j):
        return (t + j) % 4

    def features(q, size):
        return pl.ds(pl.multiple_of(q * size, size), size)

    loads = [
        pltpu.make_async_copy(a, b, sem_local.at[3 + n])
        for n, (a, b) in enumerate(
            [
                (normed, nb),
                (sgate_hbm, sgate),
                (sup_hbm, sup),
                (sdown_hbm, sdown),
                (proj_in, proj),
                (gate_hbm, gate),
                (up_hbm, up),
            ]
        )
    ]
    barrier = pltpu.get_barrier_semaphore()
    for i in range(1, 32):
        pl.semaphore_signal(barrier, inc=1, device_id={"ep": ahead(i)}, device_id_type=MESH)
    for j in range(1, 4):
        pl.semaphore_signal(barrier, inc=1, device_id={"tp": column(j)}, device_id_type=MESH)
    pl.semaphore_wait(barrier, 34)

    def weight_copy(j):
        return pltpu.make_async_remote_copy(
            src_ref=down.at[:, features(column(j), width)],
            dst_ref=wdn.at[features(t, units), :],
            send_sem=ws.at[j],
            recv_sem=wr.at[j],
            device_id={"tp": column(j)},
            device_id_type=MESH,
        )

    own_weight = pltpu.make_async_copy(
        down.at[:, features(t, width)], wdn.at[features(t, units), :], sem_local.at[0]
    )
    own_rows = pltpu.make_async_copy(
        outbox.at[me], inbox.at[pl.ds(0, rows), mine], sem_local.at[1]
    )

    def dispatch(i):
        return pltpu.make_async_remote_copy(
            src_ref=outbox.at[ahead(i)],
            dst_ref=inbox.at[pl.ds(i * rows, rows), mine],
            send_sem=ds.at[i],
            recv_sem=dr.at[i],
            device_id={"ep": ahead(i)},
            device_id_type=MESH,
        )

    def to_corner(n):
        dz, dy = PAIRS[n]
        start = ((z + dz) % 4) * 8 + ((y + dy) % 4) * 2
        k = TURNS.index(n)
        leg = legs(n)[0]
        return pltpu.make_async_remote_copy(
            src_ref=outbox.at[pl.ds(start, 2)],
            dst_ref=corner.at[k],
            send_sem=ks.at[k],
            recv_sem=kr.at[k],
            device_id={"ep": away(*leg, 0)},
            device_id_type=MESH,
        )

    def from_corner(i):
        k = TURNS.index(i // 2)
        leg = legs(i // 2)[1]
        return pltpu.make_async_remote_copy(
            src_ref=corner.at[k, (c + i % 2) % 2],
            dst_ref=inbox.at[pl.ds(i * rows, rows), mine],
            send_sem=ds.at[i],
            recv_sem=dr.at[i],
            device_id={"ep": away(*leg, i % 2)},
            device_id_type=MESH,
        )

    def arrival(i):
        return from_corner(i) if i // 2 in TURNS else dispatch(i)

    def back_to_corner(n):
        k = TURNS.index(n)
        leg = legs(n)[0]
        return pltpu.make_async_remote_copy(
            src_ref=outs.at[pl.ds(n * 2 * rows, 2 * rows), :],
            dst_ref=corner_back.at[k],
            send_sem=bs.at[k],
            recv_sem=br.at[k],
            device_id={"ep": away(-leg[0], -leg[1], 0)},
            device_id_type=MESH,
        )

    def back_from_corner(i):
        k = TURNS.index(i // 2)
        one, two = legs(i // 2)
        return pltpu.make_async_remote_copy(
            src_ref=corner_back.at[k, pl.ds((i % 2) * rows, rows)],
            dst_ref=ret.at[away(*one, 0)],
            send_sem=rs.at[i],
            recv_sem=rr.at[i],
            device_id={"ep": away(-two[0], -two[1], i % 2)},
            device_id_type=MESH,
        )

    def return_leg(i):
        return back_from_corner(i) if i // 2 in TURNS else give_back(i)

    def forward(i):
        place = inbox.at[pl.ds(i * rows, rows), lacking]
        return pltpu.make_async_remote_copy(
            src_ref=place,
            dst_ref=place,
            send_sem=fs.at[i],
            recv_sem=fr.at[i],
            device_id={"tp": column(1 if i % 2 == 0 else 3)},
            device_id_type=MESH,
        )

    def hidden_copy(g, j):
        to = j
        source = t
        if j == 2:
            to = 1 if g % 2 == 0 else 3
            source = column(4 - to)
        place = hid.at[pl.ds(g * group, group), features(source, units)]
        return pltpu.make_async_remote_copy(
            src_ref=place,
            dst_ref=place,
            send_sem=hs.at[g, j],
            recv_sem=hr.at[g, j],
            device_id={"tp": column(to)},
            device_id_type=MESH,
        )

    def give_back(i):
        return pltpu.make_async_remote_copy(
            src_ref=outs.at[pl.ds(i * rows, rows), :],
            dst_ref=ret.at[me],
            send_sem=rs.at[i],
            recv_sem=rr.at[i],
            device_id={"ep": behind(i)},
            device_id_type=MESH,
        )

    own_back = pltpu.make_async_copy(outs.at[pl.ds(0, rows), :], ret.at[me], sem_local.at[2])

    own_rows.start()
    dispatch(1).start()
    straight = list(STRAIGHT)
    for count, n in enumerate(TURNS):
        to_corner(n).start()
        if count % 3 == 0:
            for _ in range(2):
                m = straight.pop(0)
                dispatch(2 * m).start()
                dispatch(2 * m + 1).start()
    own_weight.start()
    for j in range(1, 4):
        weight_copy(j).start()
    for load in loads:
        load.start()

    length, channels = value_in.shape
    edge = rim.shape[0]
    tap_count = taps.shape[0]
    block = length // 4
    wide = nb.shape[1]

    rim_copy = pltpu.make_async_remote_copy(
        src_ref=rim_out,
        dst_ref=rim,
        send_sem=cs.at[0],
        recv_sem=cr.at[0],
        device_id={"ep": (me + 1) % 32},
        device_id_type=MESH,
    )

    def stats_copy(j):
        return pltpu.make_async_remote_copy(
            src_ref=stats.at[t],
            dst_ref=stats.at[t],
            send_sem=ss.at[j],
            recv_sem=sr.at[j],
            device_id={"tp": column(j)},
            device_id_type=MESH,
        )

    def tiles(count, size, body):
        def step(k, carry):
            body(pl.ds(pl.multiple_of(k * size, size), size))
            return carry

        lax.fori_loop(0, count, step, 0)

    def gated_tile(span):
        g = gate_in[span, :].astype(F32)
        v = value_in[span, :].astype(F32) * (1.0 / (1.0 + jnp.exp(-g)))
        padded[pl.ds(pl.multiple_of(span.start + edge, edge), 64), :] = v.astype(BF).astype(F32)

    tiles(length // 64, 64, gated_tile)
    rim_out[...] = padded[length : length + edge, :].astype(BF)
    rim_copy.start()

    def shared_expert():
        for load in loads[:4]:
            load.wait()
        acc[...] = jnp.zeros_like(acc)

        def inner(ks):
            x = nb[:, ks]
            acc[:, 0:units] += jnp.dot(x, sgate[ks, :], preferred_element_type=F32)
            acc[:, units : 2 * units] += jnp.dot(x, sup[ks, :], preferred_element_type=F32)

        tiles(depth // 1024, 1024, inner)
        a = acc[:, 0:units]
        shid[...] = (a * (1.0 / (1.0 + jnp.exp(-a))) * acc[:, units : 2 * units]).astype(BF)

        def outer(ks):
            r = jnp.dot(shid[...], sdown[:, ks], preferred_element_type=F32).astype(BF)
            for b in range(4):
                part[b, block : 2 * block, ks] = r[b * block : (b + 1) * block, :]

        tiles(wide // 512, 512, outer)

    def convolve():
        rim_copy.wait_recv()
        padded[0:edge, :] = jnp.where(me == 0, 0.0, rim[...].astype(F32))

        def strip(k, carry):
            for q in range(channels // 128):
                cols = slice(128 * q, 128 * q + 128)
                window = padded[pl.ds(pl.multiple_of(k * 64, 64), 64 + edge), cols]
                total = jnp.zeros((64, 128), F32) + conv_bias[:, cols]
                for rest in range(8):
                    turned = window[rest : rest + 56 + edge, :] if rest else window
                    for tap in range(tap_count):
                        at = edge + 1 - tap_count + tap
                        if at % 8 == rest:
                            base = at - rest
                            total = total + taps[tap : tap + 1, cols] * turned[base : base + 64, :]
                filt[pl.ds(pl.multiple_of(k * 64, 64), 64), cols] = total
            return carry

        lax.fori_loop(0, length // 64, strip, 0)
        lane = lax.broadcasted_iota(jnp.int32, (128, 128), 1)
        for b in range(length // 128):
            rs_ = slice(128 * b, 128 * b + 128)
            f = filt[rs_, :]
            both = jnp.where(
                lane == 0,
                jnp.sum(f, axis=1, keepdims=True),
                jnp.where(lane == 1, jnp.sum(f * f, axis=1, keepdims=True), 0.0),
            )
            stats[t, :, rs_] = both.T[0:8, :]
        for j in range(1, 4):
            stats_copy(j).start()

    def activate():
        for j in range(1, 4):
            stats_copy(j).wait_recv()
        whole = 4.0 * channels
        for b in range(length // 128):
            rs_ = slice(128 * b, 128 * b + 128)
            total = (stats[0, :, rs_] + stats[1, :, rs_]) + (stats[2, :, rs_] + stats[3, :, rs_])
            turned = jnp.concatenate([total, jnp.zeros((120, 128), F32)], axis=0).T
            average = turned[:, 0:1] / whole
            variance = turned[:, 1:2] / whole - average * average
            v = (filt[rs_, :] - average) * lax.rsqrt(variance + EPSILON) * ln_gain[...] + ln_bias[
                ...
            ]
            act[rs_, :] = (v / (1.0 + jnp.exp(-v))).astype(BF)

    def mix():
        loads[4].wait()

        def outer(ks):
            r = jnp.dot(act[...], proj[:, ks], preferred_element_type=F32).astype(BF)
            for b in range(4):
                part[b, 0:block, ks] = r[b * block : (b + 1) * block, :]

        tiles(wide // 512, 512, outer)

    wing = wide // 2
    right, left, across = column(1), column(3), column(2)

    piece = block // 2

    def reduce_copy(n):
        if n < 4:
            span = pl.ds((n // 2) * block, block)
            source = part.at[across, span, pl.ds(n % 2 * wing, wing)]
            target = first.at[n % 2, span]
        else:
            span = pl.ds((n // 2 - 2) * piece, piece)
            source = part.at[right if n % 2 == 0 else left, span]
            target = second.at[n % 2, span]
        return pltpu.make_async_remote_copy(
            src_ref=source,
            dst_ref=target,
            send_sem=qs.at[n],
            recv_sem=qr.at[n],
            device_id={"tp": right if n % 2 == 0 else left},
            device_id_type=MESH,
        )

    def reduce_start(which):
        reduce_copy(2 * which).start()
        reduce_copy(2 * which + 1).start()

    def reduce_pass(q):
        if q % 2 == 0:
            reduce_copy(q).wait_recv()
            reduce_copy(q + 1).wait_recv()
        span = pl.ds(q * piece, piece)
        for n, owner in ((0, right), (1, left)):
            for k in range(wing // 512):
                cols = slice(n * wing + 512 * k, n * wing + 512 * k + 512)
                part[owner, span, cols] = (
                    part[owner, span, cols].astype(F32)
                    + first[n, span, 512 * k : 512 * k + 512].astype(F32)
                ).astype(BF)
            reduce_copy(2 * q + 4 + n).start()

    def reduce_end():
        for n in range(4, 12):
            reduce_copy(n).wait_recv()

        def body(ks):
            second[0, :, ks] = (
                part[t, :, ks].astype(F32)
                + second[0, :, ks].astype(F32)
                + second[1, :, ks].astype(F32)
            ).astype(BF)

        tiles(wide // 512, 512, body)
        result[0].start()

    result = [
        pltpu.make_async_copy(second.at[0, pl.ds(0, block)], mixer_out, sem_local.at[10]),
        pltpu.make_async_copy(sdown.at[pl.ds(0, block)], experts_out, sem_local.at[11]),
    ]

    load_spread = pltpu.make_async_copy(
        spread, proj.at[:, pl.ds(0, spread.shape[1])], sem_local.at[12]
    )

    def quarter_copy(j):
        return pltpu.make_async_remote_copy(
            src_ref=nb.at[pl.ds(pl.multiple_of(column(j) * block, block), block), pl.ds(0, width)],
            dst_ref=sdown.at[pl.ds(0, block), features(t, width)],
            send_sem=xs.at[j],
            recv_sem=xr.at[j],
            device_id={"tp": column(j)},
            device_id_type=MESH,
        )

    def combine(j):
        span = pl.ds(pl.multiple_of(column(j) * block, block), block)
        slots = hid.shape[0]
        for k in range(2):
            cols = slice(k * width // 2, (k + 1) * width // 2)
            values = ret[:, :, cols].reshape(slots, width // 2)
            total = jnp.dot(
                proj[span, 0:slots], values, preferred_element_type=F32
            ) + jnp.dot(proj[span, slots : 2 * slots], values, preferred_element_type=F32)
            nb[span, cols] = total.astype(BF)

    def finish():
        for j in (2, 1, 3):
            combine(j)
            quarter_copy(j).start()
        combine(0)
        own = nb[pl.ds(pl.multiple_of(t * block, block), block), 0:width]
        sdown[0:block, features(t, width)] = own

    def last_sum():
        for j in range(1, 4):
            quarter_copy(j).wait_recv()

        def body(cols):
            sdown[0:block, cols] = (
                second[0, block : 2 * block, cols].astype(F32) + sdown[0:block, cols].astype(F32)
            ).astype(BF)

        tiles(wide // 512, 512, body)
        result[1].start()

    def receive(g):
        for i in range(8 * g, 8 * g + 8):
            if i == 0:
                own_rows.wait()
            else:
                arrival(i).wait_recv()
            forward(i).start()

    def hidden(g):
        for i in range(8 * g, 8 * g + 8):
            forward(i).wait_recv()
        span = pl.ds(g * group, group)
        acc[...] = jnp.zeros_like(acc)

        def body(ks):
            x = inbox[span, ks]
            acc[0:group, 0:units] += jnp.dot(x, gate[ks, :], preferred_element_type=F32)
            acc[0:group, units : 2 * units] += jnp.dot(x, up[ks, :], preferred_element_type=F32)

        tiles(depth // 1024, 1024, body)
        a = acc[0:group, 0:units]
        hid[span, features(t, units)] = (
            a * (1.0 / (1.0 + jnp.exp(-a))) * acc[0:group, units : 2 * units]
        ).astype(BF)
        hidden_copy(g, 1).start()
        hidden_copy(g, 3).start()

    def pass_hidden(g):
        hidden_copy(g, 1).wait_recv()
        hidden_copy(g, 3).wait_recv()
        hidden_copy(g, 2).start()

    def project(g):
        hidden_copy(g, 2).wait_recv()
        span = pl.ds(g * group, group)
        step = 256

        def body(k, carry):
            ks = pl.ds(pl.multiple_of(k * step, step), step)
            outs[span, ks] = jnp.dot(
                hid[span, :], wdn[:, ks], preferred_element_type=F32
            ).astype(BF)
            return carry

        lax.fori_loop(0, width // step, body, 0)
        for n in range(4 * g, 4 * g + 4):
            if n in TURNS:
                back_to_corner(n).start()
            else:
                if n == 0:
                    own_back.start()
                else:
                    give_back(2 * n).start()
                give_back(2 * n + 1).start()

    def turn(ks_):
        for k in ks_:
            to_corner(TURNS[k]).wait_recv()
            from_corner(2 * TURNS[k]).start()
            from_corner(2 * TURNS[k] + 1).start()

    def turn_back(g):
        for n in range(4 * g, 4 * g + 4):
            if n in TURNS:
                back_to_corner(n).wait_recv()
                back_from_corner(2 * n).start()
                back_from_corner(2 * n + 1).start()

    shared_expert()
    reduce_start(1)
    turn(range(0, 2))
    convolve()
    turn(range(2, 4))
    receive(0)
    activate()
    turn(range(4, 6))
    mix()
    load_spread.start()
    turn(range(6, 9))
    reduce_start(0)
    receive(1)
    loads[5].wait()
    loads[6].wait()
    hidden(0)
    receive(2)
    pass_hidden(0)
    hidden(1)
    own_weight.wait()
    for j in range(1, 4):
        weight_copy(j).wait()
    project(0)
    receive(3)
    pass_hidden(1)
    hidden(2)
    reduce_pass(2)
    project(1)
    pass_hidden(2)
    hidden(3)
    turn_back(1)
    project(2)
    pass_hidden(3)
    reduce_pass(3)
    project(3)
    reduce_pass(0)
    reduce_pass(1)
    turn_back(2)
    turn_back(3)
    own_back.wait()
    for i in range(1, 32):
        return_leg(i).wait_recv()
    load_spread.wait()
    finish()
    reduce_end()
    last_sum()

    rim_copy.wait_send()
    for j in range(1, 4):
        stats_copy(j).wait_send()
    for n in range(12):
        reduce_copy(n).wait_send()
    result[0].wait()
    for i in range(1, 32):
        arrival(i).wait_send()
    for n in TURNS:
        to_corner(n).wait_send()
        back_to_corner(n).wait_send()
    for i in range(32):
        forward(i).wait_send()
    for g in range(4):
        for j in range(1, 4):
            hidden_copy(g, j).wait_send()
    for i in range(1, 32):
        return_leg(i).wait_send()
    for j in range(1, 4):
        quarter_copy(j).wait_send()
    result[1].wait()


def norm_kernel(table, tokens, gain, tables, normed, sends, receives):
    t = lax.axis_index("tp")
    barrier = pltpu.get_barrier_semaphore()
    for j in range(1, 4):
        pl.semaphore_signal(barrier, inc=1, device_id={"tp": (t + j) % 4}, device_id_type=MESH)
    pl.semaphore_wait(barrier, 3)

    def table_copy(j):
        return pltpu.make_async_remote_copy(
            src_ref=table,
            dst_ref=tables.at[t],
            send_sem=sends.at[j],
            recv_sem=receives.at[j],
            device_id={"tp": (t + j) % 4},
            device_id_type=MESH,
        )

    for j in range(1, 4):
        table_copy(j).start()
    tables[t] = table[...]
    size = 32

    def body(k, carry):
        span = pl.ds(pl.multiple_of(k * size, size), size)
        x = tokens[span, :].astype(F32)
        scale = lax.rsqrt(jnp.mean(x * x, axis=1, keepdims=True) + EPSILON)
        normed[span, :] = (x * scale * gain[...]).astype(BF)
        return carry

    lax.fori_loop(0, tokens.shape[0] // size, body, 0)
    for j in range(1, 4):
        table_copy(j).wait()


def normed_rows(table, tokens, gain):
    vmem = pl.BlockSpec(memory_space=pltpu.VMEM)
    return pl.pallas_call(
        norm_kernel,
        out_shape=(
            jax.ShapeDtypeStruct((4, *table.shape), F32),
            jax.ShapeDtypeStruct(tokens.shape, BF),
        ),
        in_specs=[vmem] * 3,
        out_specs=(vmem, vmem),
        scratch_shapes=[pltpu.SemaphoreType.DMA((4,)), pltpu.SemaphoreType.DMA((4,))],
        compiler_params=pltpu.CompilerParams(
            collective_id=1, has_side_effects=True, vmem_limit_bytes=24 * 1024 * 1024
        ),
    )(table, tokens, gain[None, :])


def routed_rows(outbox, normed, mixer, weights, spread):
    count, rows, sent = outbox.shape
    depth, units = weights[0].shape
    width = weights[2].shape[1] // 4
    total = count * rows
    length, channels = mixer[0].shape
    wide = weights[2].shape[1]
    block = length // 4
    dma = pltpu.SemaphoreType.DMA
    vmem = pl.BlockSpec(memory_space=pltpu.VMEM)
    hbm = pl.BlockSpec(memory_space=pl.ANY)
    return pl.pallas_call(
        expert_kernel,
        out_shape=(
            jax.ShapeDtypeStruct((block, wide), BF),
            jax.ShapeDtypeStruct((block, wide), BF),
            jax.ShapeDtypeStruct((len(TURNS), 2, rows, sent), BF),
            jax.ShapeDtypeStruct((len(TURNS), 2 * rows, width), BF),
        ),
        in_specs=[hbm, hbm] + [vmem] * 6 + [hbm] * 8,
        out_specs=(hbm,) * 4,
        scratch_shapes=[
            pltpu.VMEM((total, depth), BF),
            pltpu.VMEM((total, 4 * units), BF),
            pltpu.VMEM((4 * units, width), BF),
            pltpu.VMEM((total, width), BF),
            pltpu.VMEM((length, 2 * units), F32),
            pltpu.VMEM((depth, units), BF),
            pltpu.VMEM((depth, units), BF),
            pltpu.VMEM((length + 32, channels), F32),
            pltpu.VMEM((length, channels), F32),
            pltpu.VMEM((length, channels), BF),
            pltpu.VMEM((32, channels), BF),
            pltpu.VMEM((32, channels), BF),
            pltpu.VMEM((4, 8, length), F32),
            pltpu.VMEM((channels, wide), BF),
            pltpu.VMEM((length, wide), BF),
            pltpu.VMEM((depth, units), BF),
            pltpu.VMEM((depth, units), BF),
            pltpu.VMEM((units, wide), BF),
            pltpu.VMEM((length, units), BF),
            pltpu.VMEM((4, 2 * block, wide), BF),
            pltpu.VMEM((2, 2 * block, wide // 2), BF),
            pltpu.VMEM((2, 2 * block, wide), BF),
            pltpu.VMEM((count, rows, width), BF),
            dma((13,)),
            dma((4,)),
            dma((4,)),
            dma((1,)),
            dma((1,)),
            dma((4,)),
            dma((4,)),
            dma((12,)),
            dma((12,)),
            dma((32,)),
            dma((32,)),
            dma((32,)),
            dma((32,)),
            dma((4, 4)),
            dma((4, 4)),
            dma((4,)),
            dma((4,)),
            dma((32,)),
            dma((32,)),
            dma((9,)),
            dma((9,)),
            dma((9,)),
            dma((9,)),
        ],
        compiler_params=pltpu.CompilerParams(
            collective_id=0, has_side_effects=True, vmem_limit_bytes=67_043_328
        ),
    )(outbox, normed, *mixer, *weights, spread)


def per_device(
    value_in,
    gate_in,
    conv_taps,
    conv_bias,
    ln_gain,
    ln_bias,
    out_proj,
    tokens_b,
    norm_gain,
    routes,
    route_weights,
    expert_gate,
    expert_up,
    expert_down,
    shared_gate,
    shared_up,
    shared_down,
):
    tp_count = lax.axis_size("tp")
    ep_count = lax.axis_size("ep")
    t = lax.axis_index("tp")
    rows_own, top_count = routes.shape
    rows_all = rows_own * tp_count
    model_width = tokens_b.shape[1]

    own = jnp.concatenate(
        [
            routes.astype(F32).T,
            route_weights.T,
            jnp.zeros((8 - 2 * top_count, rows_own), F32),
        ],
        axis=0,
    )
    tables, normed_b = normed_rows(own, tokens_b, norm_gain)
    chosen = jnp.swapaxes(tables[:, 0:top_count, :], 1, 2).astype(jnp.int32)
    weights = jnp.swapaxes(tables[:, top_count : 2 * top_count, :], 1, 2)
    weights = weights.reshape(rows_all, top_count)
    onehot = chosen[:, :, :, None] == jnp.arange(ep_count, dtype=jnp.int32)
    named = jnp.sum(onehot.astype(F32), axis=2).astype(BF)
    ranks = jnp.arange(rows_own, dtype=jnp.int32)
    lower = (ranks[:, None] > ranks[None, :]).astype(BF)
    earlier = jnp.einsum("ij,bje->bie", lower, named, preferred_element_type=F32)
    places = jnp.sum(jnp.where(onehot, earlier[:, :, None, :], 0.0), axis=3).astype(jnp.int32)
    slots = (
        chosen * (tp_count * CAP)
        + jnp.arange(tp_count, dtype=jnp.int32)[:, None, None] * CAP
        + places
    ).reshape(rows_all, top_count)
    slot_count = ep_count * tp_count * CAP

    sent = model_width - EDGE
    part = lax.dynamic_slice_in_dim(normed_b, (1 - t % 2) * EDGE, sent, 1)
    ids = jnp.arange(slot_count, dtype=jnp.int32)
    select = (
        (ids[:, None] == slots[None, :, 0]) | (ids[:, None] == slots[None, :, 1])
    ).astype(BF)
    outbox = jnp.dot(select, part, preferred_element_type=F32).astype(BF)
    outbox = outbox.reshape(ep_count, tp_count * CAP, sent)

    spread = jnp.where(ids[None, :] == slots[:, 0:1], weights[:, 0:1], 0.0) + jnp.where(
        ids[None, :] == slots[:, 1:2], weights[:, 1:2], 0.0
    )
    high = spread.astype(BF)
    low = (spread - high.astype(F32)).astype(BF)
    mixer_rows, expert_rows, _, _ = routed_rows(
        outbox,
        normed_b,
        (
            value_in,
            gate_in,
            conv_taps,
            conv_bias[None, :],
            ln_gain[None, :],
            ln_bias[None, :],
            out_proj,
        ),
        (
            expert_gate[0],
            expert_up[0],
            expert_down[0],
            shared_gate,
            shared_up,
            shared_down,
        ),
        jnp.concatenate([high, low], axis=1),
    )
    return (mixer_rows, expert_rows)


def solution(mesh):
    return jax.shard_map(
        per_device,
        mesh=mesh,
        in_specs=(
            P("ep", "tp"),
            P("ep", "tp"),
            P(None, "tp"),
            P("tp"),
            P("tp"),
            P("tp"),
            P("tp", None),
            P("ep", None),
            P(),
            P(("ep", "tp"), None),
            P(("ep", "tp"), None),
            P("ep", None, "tp"),
            P("ep", None, "tp"),
            P("ep", "tp", None),
            P(None, "tp"),
            P(None, "tp"),
            P("tp", None),
        ),
        out_specs=(P(("ep", "tp"), None), P(("ep", "tp"), None)),
        check_vma=False,
    )
```
